32 devices in a mesh: sp: 16 (over z, y, x), tp: 2 (over core).
Axes of the slice: x: 2, y: 2, z: 4, core: 2. Of those that a mesh axis runs over, the one named last changes fastest.
Arguments:
- resid: bfloat16 [8192, 2048], P('sp'), may hold values from -6 to 6
- queries: bfloat16 [8192, 2048], P('sp', 'tp'), may hold values from -6 to 6
- keys: bfloat16 [8192, 512], P('sp', 'tp'), may hold values from -6 to 6
- values: bfloat16 [8192, 512], P('sp', 'tp'), may hold values from -6 to 6
- documents: int32 [8192], P('sp'), may hold values from 0 to 7, never falling along the last dimension, each value on 1 to 2048 neighbouring positions
- q_gain: float32 [64], replicated, may hold values from 0.5 to 6.5
- k_gain: float32 [64], replicated, may hold values from 0.5 to 6.5
- sink: float32 [32], P('tp'), may hold values from -1 to 5
- w_out: bfloat16 [2048, 2048], P('tp'), may hold values from -0.5 to 0.5
- n_gain: float32 [2048], replicated, may hold values from 0.1 to 1.9
- w_up: bfloat16 [2048, 8192], P('sp', 'tp'), may hold values from -0.125 to 0.125
- w_down: bfloat16 [8192, 2048], P('tp', 'sp'), may hold values from -0.0625 to 0.0625
Outputs:
- layer_out: bfloat16 [8192, 2048], P('sp')
The draws below stay inside these ranges and needn't reach their ends.
All inputs are finite; a program needn't handle non-finite values.
Results may differ from the reference program's by a relative error of at most 0.018.
The reference program's roundings to bfloat16 on the way count: a program that leaves them out, or rounds other values in their place, can miss the bound.
Values may be sent and summed in bfloat16 or wider, within the bound.
A program may use at most 128 MiB of HBM per device.

```python
import math
import jax
import jax.numpy as jnp
import numpy as np
from jax import lax

D = 2048
HEADS = 32
KV_HEADS = 8
HEAD = 64
FF = 8192
WINDOW = 128
TOK_DEV = 512
TOKENS = 8192
N_SP = 16
N_TP = 2


def base_keys(key):
    return jax.random.normal(jax.random.fold_in(key, 3), (TOKENS, KV_HEADS * HEAD), jnp.float32)


def draw_keys(key, part):
    drawn = base_keys(key)
    return jnp.clip(drawn, -6.0, 6.0).astype(jnp.bfloat16)


def draw_queries(key, part):
    drawn = jax.random.normal(jax.random.fold_in(key, 7), (TOKENS, HEADS * HEAD), jnp.float32)
    return jnp.clip(drawn, -6.0, 6.0).astype(jnp.bfloat16)


def draw_q_gain(key, part):
    return jax.random.uniform(jax.random.fold_in(key, 21), (HEAD,), jnp.float32, 0.5, 1.5)


def draw_k_gain(key, part):
    return jax.random.uniform(jax.random.fold_in(key, 23), (HEAD,), jnp.float32, 0.5, 1.5)


def block_levels(key, shape, cuts, least, top_value):
    level, own = 1.0, jax.random.fold_in(key, 6)
    for position, shards_of in cuts:
        draws = jnp.exp(jax.random.uniform(jax.random.fold_in(own, position), (shards_of,), jnp.float32, least / len(cuts), top_value / len(cuts)))
        level = level * jnp.repeat(draws, shape[position] // shards_of).reshape([-1 if axis == position else 1 for axis in range(len(shape))])
    return level


def profile(number_of, total, bound, lean):
    loads = [(1 << 20) // math.isqrt(rank ** lean) + 1 for rank in range(2, number_of + 1)]
    rest, holding = total - bound - (number_of - 1), [1] * (number_of - 1)
    while rest > 0:
        candidates = [i for i in range(number_of - 1) if holding[i] < bound]
        mass, budget = sum([loads[i] for i in candidates]), rest
        for i in candidates:
            extra = min(bound - holding[i], max(1, budget * loads[i] // mass), rest)
            holding[i] = holding[i] + extra
            rest = rest - extra
    return np.array([bound] + holding)


def uneven(key, amount, total, limit, lean):
    if amount == 2:
        one = jax.random.randint(key, (), max(1, total - limit), min(limit, total - 1) + 1)
        return jnp.stack([one, total - one])
    sizes = jnp.asarray(profile(amount, total, limit, lean), jnp.int32)
    twos = (amount - 1) // 2
    source_of, taker = sizes[1:1 + 2 * twos:2], sizes[2:2 + 2 * twos:2]
    slack = jnp.minimum(source_of - 1, limit - taker)
    passed = jax.random.randint(jax.random.fold_in(key, 1), (twos,), 0, 1 << 20) % (slack + 1)
    sizes = sizes.at[1:1 + 2 * twos:2].set(source_of - passed).at[2:2 + 2 * twos:2].set(taker + passed)
    return sizes[jax.random.permutation(jax.random.fold_in(key, 2), amount)]


def gaussian(stream_key, extent, deviation, bound, cuts=(), kind=jnp.bfloat16):
    result = jax.random.normal(stream_key, extent, jnp.float32) * deviation
    if len(cuts) > 0:
        result = block_levels(stream_key, extent, cuts, -0.22, 0.18) * result
    return jnp.clip(result, min=-bound, max=bound).astype(kind)


def setup_inputs(seed: int = 0) -> dict:
    splits = jax.random.split(jax.random.key(seed), 13)
    resid = gaussian(splits[0], (TOKENS, D), 1.0, 6.0, ((0, 16),))
    queries = draw_queries(jax.random.fold_in(splits[12], 71), 0)
    keys = draw_keys(jax.random.fold_in(splits[12], 71), 0)
    values = gaussian(splits[3], (TOKENS, KV_HEADS * HEAD), 1.0, 6.0, ((0, 16), (1, 2)))
    documents = jnp.searchsorted(jnp.cumsum(uneven(splits[4], N_SP // 2, TOKENS, 4 * TOK_DEV, 0)), jnp.arange(TOKENS), side="right").astype(jnp.int32)
    q_gain = draw_q_gain(jax.random.fold_in(splits[12], 71), 0)
    k_gain = draw_k_gain(jax.random.fold_in(splits[12], 71), 0)
    sink = jnp.clip(-1.0 + 6.0 * jax.random.uniform(splits[7], (HEADS,), jnp.float32) ** block_levels(splits[7], (HEADS,), ((0, 2),), -0.2, 0.2), -1.0, 5.0)
    w_out = gaussian(splits[8], (HEADS * HEAD, D), (HEADS * HEAD // 16) ** -0.5, 0.5, ((0, 2),))
    n_gain = jnp.clip(1.0 + 0.18 * jax.random.normal(splits[9], (D,), jnp.float32), 0.1, 1.9)
    w_up = gaussian(splits[10], (D, FF), D ** -0.5, 0.125, ((0, 16), (1, 2)))
    w_down = gaussian(splits[11], (FF, D), FF ** -0.5, 0.0625, ((0, 2), (1, 16)))
    return dict(resid=resid, queries=queries, keys=keys, values=values, documents=documents, q_gain=q_gain, k_gain=k_gain, sink=sink, w_out=w_out, n_gain=n_gain, w_up=w_up, w_down=w_down)


EPS = 1e-06

def rms_scale(field, gain):
    wide = field.astype(jnp.float32)
    return wide * lax.rsqrt(lax.optimization_barrier(jnp.mean(wide * wide, axis=-1, keepdims=True)) + EPS) * gain.astype(jnp.float32)

def reference(resid, queries, keys, values, documents, q_gain, k_gain, sink, w_out, n_gain, w_up, w_down):
    group = HEADS // KV_HEADS
    qnorm = rms_scale(queries.reshape(TOKENS, KV_HEADS, group, HEAD), q_gain).astype(jnp.bfloat16)
    knorm = rms_scale(keys.reshape(TOKENS, KV_HEADS, HEAD), k_gain).astype(jnp.bfloat16)
    vheads = values.reshape(TOKENS, KV_HEADS, HEAD)
    padding = ((WINDOW, WINDOW), (0, 0), (0, 0))
    key_pad = jnp.pad(knorm, padding)
    value_pad = jnp.pad(vheads, padding)
    doc_pad = jnp.pad(documents, (WINDOW, WINDOW), constant_values=-1)
    slopes = jnp.exp2(-8.0 * (jnp.arange(HEADS, dtype=jnp.float32) + 1.0) / HEADS).reshape(KV_HEADS, group)
    sink_f = sink.astype(jnp.float32).reshape(KV_HEADS, group)
    span = TOK_DEV
    blocks = TOKENS // span
    query_blocks = qnorm.reshape(blocks, span, KV_HEADS, group, HEAD)
    doc_blocks = documents.reshape(blocks, span)

    def one_block(args):
        qblock, dblock, number = args
        start = number * span
        kblock = lax.dynamic_slice_in_dim(key_pad, start, span + 2 * WINDOW, 0)
        vblock = lax.dynamic_slice_in_dim(value_pad, start, span + 2 * WINDOW, 0)
        dkeys = lax.dynamic_slice_in_dim(doc_pad, start, span + 2 * WINDOW, 0)
        query_pos = start + jnp.arange(span, dtype=jnp.int32)
        key_pos = start - WINDOW + jnp.arange(span + 2 * WINDOW, dtype=jnp.int32)
        distance = key_pos[None, :] - query_pos[:, None]
        allowed = (jnp.abs(distance) <= WINDOW) & (key_pos[None, :] >= 0) & (key_pos[None, :] < TOKENS)
        allowed = allowed & (dkeys[None, :] == dblock[:, None])
        scores = jnp.einsum('rkgd,skd->kgrs', qblock.astype(jnp.float32), kblock.astype(jnp.float32)) * HEAD ** (-0.5)
        scores = scores - slopes[:, :, None, None] * jnp.abs(distance).astype(jnp.float32)[None, None]
        scores = jnp.where(allowed[None, None], scores, jnp.float32(-1e+30))
        highest = jnp.maximum(lax.optimization_barrier(jnp.max(scores, axis=-1)), sink_f[:, :, None])
        weights = jnp.exp(scores - highest[..., None])
        denom = lax.optimization_barrier(jnp.sum(weights, axis=-1)) + jnp.exp(sink_f[:, :, None] - highest)
        rounded = weights.astype(jnp.bfloat16)
        summed = jnp.einsum('kgrs,skd->rkgd', rounded.astype(jnp.float32), vblock.astype(jnp.float32))
        return (summed / denom.transpose(2, 0, 1)[..., None]).astype(jnp.bfloat16)
    attended = lax.map(one_block, (query_blocks, doc_blocks, jnp.arange(blocks, dtype=jnp.int32)))
    attended = attended.reshape(TOKENS, HEADS * HEAD)
    cols = HEADS * HEAD // N_TP
    head_mix = jnp.zeros((TOKENS, D), jnp.float32)
    for index in range(N_TP):
        partial_sum = jnp.dot(attended[:, index * cols:(index + 1) * cols], w_out[index * cols:(index + 1) * cols], preferred_element_type=jnp.float32)
        head_mix = head_mix + partial_sum.astype(jnp.bfloat16).astype(jnp.float32)
    middle = (resid.astype(jnp.float32) + head_mix).astype(jnp.bfloat16)
    normed = rms_scale(middle, n_gain).astype(jnp.bfloat16)
    units = FF // N_TP
    unit_mix = jnp.zeros((TOKENS, D), jnp.float32)
    for index in range(N_TP):
        upward = jnp.dot(normed, w_up[:, index * units:(index + 1) * units], preferred_element_type=jnp.float32)
        active = jnp.square(jax.nn.relu(upward)).astype(jnp.bfloat16)
        partial_sum = jnp.dot(active, w_down[index * units:(index + 1) * units], preferred_element_type=jnp.float32)
        unit_mix = unit_mix + partial_sum.astype(jnp.bfloat16).astype(jnp.float32)
    return (middle.astype(jnp.float32) + unit_mix).astype(jnp.bfloat16)
```

```python
import functools

import jax
import jax.numpy as jnp
from jax import lax
from jax.experimental import pallas as pl
from jax.experimental.pallas import tpu as pltpu
from jax.sharding import PartitionSpec as P

WINDOW = 128
EPS = 1e-06
MEMBERS = 4
F32 = jnp.float32
BF16 = jnp.bfloat16
MESH = pl.DeviceIdType.MESH


def rms(wide, gain):
    return wide * lax.rsqrt(jnp.mean(wide * wide, axis=-1, keepdims=True) + EPS) * gain


def kernel(
    n_sp,
    head,
    heads,
    kv_heads,
    slopes,
    resid,
    queries,
    keys,
    values,
    docs,
    q_gain,
    k_gain,
    sink,
    w_out,
    n_gain,
    w_up,
    w_down,
    out,
    q,
    kx,
    vx,
    dx,
    kn,
    att,
    wo,
    res,
    mixed,
    other_in,
    mid,
    normed,
    wu,
    wd,
    act,
    part,
    twin_out,
    twin_in,
    first_out,
    first_in,
    second_out,
    second_in,
    waiting,
    total,
    half_out,
    halo_send,
    halo_recv,
    w_send,
    w_recv,
    w_local,
    loc_sem,
    tok_send,
    tok_recv,
    pair_send,
    pair_recv,
    swap_send,
    swap_recv,
    twin_send,
    twin_recv,
    sum_send,
    sum_recv,
    fin_send,
    fin_recv,
    fin_local,
):
    rows = queries.shape[0]
    half = rows // 2
    depth = w_up.shape[0]
    units = wu.shape[1]
    width = wd.shape[1]
    group = heads // kv_heads
    n_za = n_sp // 8
    block = 2 * w_down.shape[1]

    sp = lax.axis_index("sp")
    t = lax.axis_index("tp")
    u = 1 - t
    x = sp % 2
    y = (sp // 2) % 2
    zb = (sp // 4) % 2
    za = sp // 8
    me = zb * 2 + x

    def index(za_, zb_, y_, x_):
        return za_ * 8 + zb_ * 4 + y_ * 2 + x_

    def flip(v, by):
        return 1 - v if by else v

    def remote(src, dst, send, recv, where):
        return pltpu.make_async_remote_copy(
            src_ref=src, dst_ref=dst, send_sem=send, recv_sem=recv,
            device_id=where, device_id_type=MESH,
        )

    own_q = pltpu.make_async_copy(queries, q, loc_sem.at[5])
    own_k = pltpu.make_async_copy(keys, kx.at[pl.ds(WINDOW, rows), :], loc_sem.at[2])
    own_v = pltpu.make_async_copy(values, vx.at[pl.ds(WINDOW, rows), :], loc_sem.at[3])
    own_d = pltpu.make_async_copy(docs, dx.at[:, pl.ds(WINDOW, rows)], loc_sem.at[4])
    own_k.start()
    own_d.start()
    own_q.start()
    own_v.start()

    up_to = lax.rem(sp + 1, n_sp)
    down_to = lax.rem(sp + n_sp - 1, n_sp)
    flips = ((0, 1), (1, 0), (1, 1))
    near = [(index(za, flip(zb, fz), y, flip(x, fx)), t) for fz, fx in flips]
    across = (index(za, zb, 1 - y, x), t)
    partners = [(sp, u), (up_to, t), (down_to, t), across] + near
    partners += [(index(lax.rem(za + d, n_za), zb, y, x), t) for d in range(1, n_za)]
    with jax.named_scope("barrier"):
        greeting = pltpu.get_barrier_semaphore()
        for where in partners:
            pl.semaphore_signal(greeting, inc=1, device_id=where, device_id_type=MESH)
        pl.semaphore_wait(greeting, len(partners))

    def halo(side, where):
        src = rows - WINDOW if side == 0 else 0
        dst = 0 if side == 0 else WINDOW + rows
        return [
            remote(keys.at[pl.ds(src, WINDOW), :], kx.at[pl.ds(dst, WINDOW), :],
                   halo_send.at[side, 0], halo_recv.at[side, 0], where),
            remote(docs.at[:, pl.ds(src, WINDOW)], dx.at[:, pl.ds(dst, WINDOW)],
                   halo_send.at[side, 2], halo_recv.at[side, 2], where),
            remote(values.at[pl.ds(src, WINDOW), :], vx.at[pl.ds(dst, WINDOW), :],
                   halo_send.at[side, 1], halo_recv.at[side, 1], where),
        ]

    @pl.when(sp < n_sp - 1)
    def _():
        for c in halo(0, (up_to, t)):
            c.start()

    @pl.when(sp > 0)
    def _():
        for c in halo(1, (down_to, t)):
            c.start()

    def place(w, s):
        if w == 0:
            return wu.at[pl.ds(pl.multiple_of(s * depth, depth), depth), :]
        return wd.at[:, pl.ds(pl.multiple_of(s * (block // 2), block // 2), block // 2)]

    def source(w, m):
        at = pl.ds(pl.multiple_of(m * units, units), units)
        return w_up.at[:, at] if w == 0 else w_down.at[at, :]

    def first_copy(w, k):
        fz, fx = flips[k]
        return remote(source(w, flip(zb, fz) * 2 + flip(x, fx)), place(w, sp), w_send.at[w, k],
                      w_recv.at[w, sp], near[k])

    locals_ = [pltpu.make_async_copy(source(w, me), place(w, sp), w_local.at[w]) for w in range(2)]

    def arrived(w, s):
        remote(place(w, s), place(w, s), w_send.at[w, 0], w_recv.at[w, s], (sp, u)).wait_recv()

    sent = [[], []]

    def start(w, s, where, src=None):
        c = remote(place(w, s) if src is None else src, place(w, s), w_send.at[w, 3 + len(sent[w])],
                   w_recv.at[w, s], where)
        c.start()
        sent[w].append(c)

    def along(w, s, src=None):
        for d in range(1, n_za):
            start(w, s, (index(lax.rem(za + d, n_za), zb, y, x), t), src)

    def member_at(k):
        fz, fx = (0, 0) if k == 0 else flips[k - 1]
        return flip(zb, fz), flip(x, fx)

    def spread(w, k):
        with jax.named_scope(f"spread#w={w}#k={k}"):
            zb_, x_ = member_at(k)
            s = index(za, zb_, y, x_)
            arrived(w, s)
            along(w, s)

    def cross(w, k):
        zb_, x_ = member_at(k)
        start(w, index(za, zb_, y, x_), across, source(w, me) if k == 0 else None)

    def relay(w, k):
        with jax.named_scope(f"relay#w={w}#k={k}"):
            zb_, x_ = member_at(k)
            for d in range(1, n_za):
                s = index(lax.rem(za + n_za - d, n_za), zb_, y, x_)
                arrived(w, s)
                start(w, s, across)

    def exchange(w):
        for k in (1, 2, 0):
            first_copy(w, k).start()
        locals_[w].start()

    exchange(0)
    along(0, sp, source(0, me))
    cross(0, 0)
    exchange(1)
    load_wo = pltpu.make_async_copy(w_out, wo, loc_sem.at[0])
    load_wo.start()
    load_res = pltpu.make_async_copy(resid.at[pl.ds(t * half, half), :], res, loc_sem.at[1])
    load_res.start()

    with jax.named_scope("own_wait"):
        own_k.wait()
        own_v.wait()
        own_d.wait()
        own_q.wait()

    @pl.when(sp > 0)
    def _():
        for c in halo(0, (down_to, t)):
            c.wait_recv()

    @pl.when(sp == 0)
    def _():
        kx[pl.ds(0, WINDOW), :] = jnp.zeros((WINDOW, kx.shape[1]), BF16)
        vx[pl.ds(0, WINDOW), :] = jnp.zeros((WINDOW, vx.shape[1]), BF16)
        dx[:, pl.ds(0, WINDOW)] = jnp.full((1, WINDOW), -1, jnp.int32)

    @pl.when(sp < n_sp - 1)
    def _():
        for c in halo(1, (up_to, t)):
            c.wait_recv()

    @pl.when(sp == n_sp - 1)
    def _():
        end = WINDOW + rows
        kx[pl.ds(end, WINDOW), :] = jnp.zeros((WINDOW, kx.shape[1]), BF16)
        vx[pl.ds(end, WINDOW), :] = jnp.zeros((WINDOW, vx.shape[1]), BF16)
        dx[:, pl.ds(end, WINDOW)] = jnp.full((1, WINDOW), -1, jnp.int32)

    def norm_keys(b, carry):
        at = pl.ds(pl.multiple_of(b * WINDOW, WINDOW), WINDOW)
        wide = kx[at, :].astype(F32)
        kn[at, :] = jnp.concatenate(
            [rms(wide[:, k * head:(k + 1) * head], k_gain[...]) for k in range(kv_heads)], axis=1
        ).astype(BF16)
        return carry

    with jax.named_scope("norm_keys"):
        lax.fori_loop(0, kx.shape[0] // WINDOW, norm_keys, 0)

    span = 3 * WINDOW
    rounds = half // WINDOW

    def attend(b, carry, to):
        at = pl.ds(pl.multiple_of(b * WINDOW, WINDOW), WINDOW)
        put = pl.ds(pl.multiple_of(to * WINDOW, WINDOW), WINDOW)
        window = pl.ds(pl.multiple_of(b * WINDOW, WINDOW), span)
        far = jnp.abs(
            lax.broadcasted_iota(jnp.int32, (WINDOW, span), 1)
            - lax.broadcasted_iota(jnp.int32, (WINDOW, span), 0) - WINDOW
        )
        own = dx[0:1, pl.ds(pl.multiple_of((b + 1) * WINDOW, WINDOW), WINDOW)].astype(F32)
        own = jnp.transpose(jnp.broadcast_to(own, (WINDOW, WINDOW)))[:, 0:1]
        allowed = (far <= WINDOW) & (dx[0:1, window].astype(F32) == own)
        mask = jnp.where(allowed, F32(0.0), F32(-1e30))
        far = far.astype(F32)
        for k in range(kv_heads):
            lanes = slice(k * head, (k + 1) * head)
            kb = kn[window, lanes]
            vb = vx[window, lanes]
            done = []
            for g in range(group):
                h = k * group + g
                slope = jnp.where(t == 0, F32(slopes[h]), F32(slopes[heads + h]))
                qb = rms(q[at, h * head:(h + 1) * head].astype(F32), q_gain[...]).astype(BF16)
                score = lax.dot_general(
                    qb, kb, (((1,), (1,)), ((), ())), preferred_element_type=F32
                ) * (head ** -0.5)
                score = (score - slope * far) + mask
                top = jnp.maximum(jnp.max(score, axis=-1, keepdims=True), sink[h])
                p = jnp.exp(score - top)
                denom = jnp.sum(p, axis=-1, keepdims=True) + jnp.exp(sink[h] - top)
                summed = jnp.dot(p.astype(BF16), vb, preferred_element_type=F32)
                done.append((summed / denom).astype(BF16))
                if len(done) == 2:
                    att[put, (h - 1) * head:(h + 1) * head] = jnp.concatenate(done, axis=1)
                    done = []
        return carry

    tile = 256
    swaps = []

    def project(r):
        lhs = att[pl.ds(r * 2 * WINDOW, 2 * WINDOW), :]

        def step(j, carry):
            cols = pl.ds(pl.multiple_of(j * tile, tile), tile)
            mixed[r, :, cols] = jnp.dot(lhs, wo[:, cols], preferred_element_type=F32).astype(BF16)
            return carry

        lax.fori_loop(0, width // tile, step, 0)

    def token_rows(slot, r):
        return normed.at[pl.ds(pl.multiple_of(slot * half + r * WINDOW, WINDOW), WINDOW), :]

    def token_copy(k, r):
        rows_ = token_rows(me * 2 + t, r)
        return remote(rows_, rows_, tok_send.at[k, r], tok_recv.at[k, r], near[k])

    def member(k):
        if k == 3:
            return me
        fz, fx = flips[k]
        return flip(zb, fz) * 2 + flip(x, fx)

    def pair_copy(k, core, r):
        rows_ = token_rows(member(k) * 2 + core, r)
        return remote(rows_, rows_, pair_send.at[k, r], pair_recv.at[k, r], (sp, u))

    def token_pass(k, r):
        with jax.named_scope(f"token#k={k}#r={r}"):
            rows_ = token_rows(member(k) * 2 + t, r)
            remote(rows_, rows_, tok_send.at[k, r], tok_recv.at[k, r], (sp, u)).wait_recv()
            if k == 1:
                token_relay(r).start()
            pair_copy(k, t, r).start()

    def token_relay(r):
        rows_ = token_rows(member(1) * 2 + t, r)
        return remote(rows_, rows_, tok_send.at[2, r], tok_recv.at[2, r], near[0])

    def one_round(r):
        with jax.named_scope("project"):
            project(r)
            swap = remote(mixed.at[r, pl.ds(pl.multiple_of(u * WINDOW, WINDOW), WINDOW), :], other_in.at[r],
                          swap_send.at[r], swap_recv.at[r], (sp, u))
            swap.start()
            swaps.append(swap)
        with jax.named_scope("swap_wait"):
            swap.wait_recv()

        def middle(i, carry):
            at = pl.ds(pl.multiple_of(i * 64, 64), 64)
            mine = pl.ds(pl.multiple_of(t * WINDOW + i * 64, 64), 64)
            here = pl.ds(pl.multiple_of(r * WINDOW + i * 64, 64), 64)
            both = mixed[r, mine, :].astype(F32) + other_in[r, at, :].astype(F32)
            value = (res[here, :].astype(F32) + both).astype(BF16)
            mid[here, :] = value
            row = pl.multiple_of((me * 2 + t) * half + r * WINDOW + i * 64, 64)
            normed[pl.ds(row, 64), :] = rms(value.astype(F32), n_gain[...]).astype(BF16)
            return carry

        with jax.named_scope("middle"):
            lax.fori_loop(0, WINDOW // 64, middle, 0)
        for k in (1, 0):
            token_copy(k, r).start()
        pair_copy(3, t, r).start()

    def attend_block(r, i):
        with jax.named_scope("attend"):
            lax.fori_loop(0, 1, lambda _, c: attend(r + i * rounds, c, 2 * r + i), 0)

    for r in range(rounds):
        attend_block(r, 0)
        if r == 0:
            spread(0, 1)
            cross(0, 1)
        attend_block(r, 1)
        if r == 0:
            for k in (2, 3):
                spread(0, k)
                cross(0, k)
            load_wo.wait()
            load_res.wait()
        one_round(r)

    def up(m):
        row = pl.multiple_of(m * rows, rows)

        def step(j, carry):
            cols = pl.ds(pl.multiple_of(j * tile, tile), tile)
            v = jnp.dot(normed[pl.ds(row, rows), :], wu[:, cols], preferred_element_type=F32)
            v = jnp.maximum(v, 0.0)
            act[pl.ds(row, rows), cols] = (v * v).astype(BF16)
            return carry

        with jax.named_scope("up"):
            lax.fori_loop(0, units // tile, step, 0)

    def pair_wait(k):
        with jax.named_scope("pair_wait"):
            for r in range(rounds):
                pair_copy(k, u, r).wait_recv()

    def finish_up():
        with jax.named_scope("finish_up"):
            locals_[0].wait()
            for a in range(n_za):
                for k in range(4):
                    arrived(0, index(a, k // 2, 1 - y, k % 2))

    along(1, sp, source(1, me))
    for k in (1, 2, 3):
        spread(1, k)
    for k in range(4):
        relay(0, k)
    for k in range(4):
        cross(1, k)
    for r in range(rounds):
        token_pass(1, r)
    finish_up()
    pair_wait(3)
    up(me)
    for r in range(rounds):
        token_pass(0, r)
    pair_wait(0)
    up(member(0))
    for r in range(rounds):
        token_pass(2, r)
    relay(1, 0)
    relay(1, 1)
    for k in (1, 2):
        pair_wait(k)
        up(member(k))
    locals_[1].wait()

    order = [(d, fz, fy) for d in range(n_za) for fy in range(2) for fz in range(2)]
    chunks = 4
    ways = ((0, 1), (1, 0))

    def block_of(p):
        d, fz, fy = order[p]
        return lax.rem(za + n_za - d, n_za) * 4 + flip(zb, fz) * 2 + flip(y, fy)

    def axes(p):
        return ways[0] if order[p][0] % 2 == 0 else ways[1]

    def cols_of(g):
        return pl.ds(pl.multiple_of(g * block, block), block)

    def twin_copy(g):
        return remote(twin_out.at[g], twin_in.at[g], twin_send.at[g], twin_recv.at[g], (sp, u))

    def first_sum(p):
        g = block_of(p)
        return remote(first_out.at[g], first_in.at[g], sum_send.at[0, g], sum_recv.at[0, g], near[axes(p)[0]])

    def second_sum(p):
        g = block_of(p)
        return remote(second_out.at[g], second_in.at[g], sum_send.at[1, g], sum_recv.at[1, g], near[axes(p)[1]])

    def down(p):
        d, fz, fy = order[p]
        g = block_of(p)
        with jax.named_scope(f"down_wait#p={p}"):
            if fy == 1:
                for i in range(2):
                    arrived(1, g * 2 + i)
        cols = cols_of(g)

        def step(c, carry):
            cz, cx = c // 2, c % 2
            row = (zb + cz - 2 * zb * cz) * 2 + (x + cx - 2 * x * cx)
            theirs = pl.ds(pl.multiple_of(row * rows + u * half, half), half)
            ours = pl.ds(pl.multiple_of(row * rows + t * half, half), half)
            twin_out[g, c, :, :] = jnp.dot(act[theirs, :], wd[:, cols], preferred_element_type=F32).astype(BF16)
            part[p % 2, c, :, :] = jnp.dot(act[ours, :], wd[:, cols], preferred_element_type=F32)
            return carry

        with jax.named_scope("down"):
            lax.fori_loop(0, chunks, step, 0)
        twin_copy(g).start()

    def combine(p):
        g = block_of(p)
        cols = cols_of(g)
        one, two = axes(p)
        with jax.named_scope("twin_wait"):
            twin_copy(g).wait_recv()

        def add(i, carry):
            at = pl.ds(pl.multiple_of(i * 64, 64), 64)

            def whole(c):
                return part[p % 2, c, at, :] + twin_in[g, c, at, :].astype(F32)

            first_out[g, 0, at, :] = whole(3).astype(BF16)
            first_out[g, 1, at, :] = whole(one + 1).astype(BF16)
            waiting[g, at, :] = whole(two + 1)
            total[g, at, :] = whole(0) + mid[at, cols].astype(F32)
            return carry

        with jax.named_scope("combine"):
            lax.fori_loop(0, half // 64, add, 0)
        first_sum(p).start()

    def merge(p):
        g = block_of(p)
        with jax.named_scope(f"merge_wait#p={p}"):
            first_sum(p).wait_recv()

        def add(i, carry):
            at = pl.ds(pl.multiple_of(i * 64, 64), 64)
            second_out[g, at, :] = (waiting[g, at, :] + first_in[g, 0, at, :].astype(F32)).astype(BF16)
            return carry

        lax.fori_loop(0, half // 64, add, 0)
        second_sum(p).start()

    def final_copies(p):
        g = block_of(p)
        cols = cols_of(g)
        mine = pl.ds(pl.multiple_of(t * half, half), half)
        return (
            pltpu.make_async_copy(half_out.at[g], out.at[mine, cols], fin_local.at[g]),
            remote(half_out.at[g], out.at[mine, cols], fin_send.at[g], fin_recv.at[g], (sp, u)),
        )

    def last(p):
        g = block_of(p)
        with jax.named_scope(f"sum_wait#p={p}"):
            second_sum(p).wait_recv()

        def add(i, carry):
            at = pl.ds(pl.multiple_of(i * 64, 64), 64)
            value = total[g, at, :] + first_in[g, 1, at, :].astype(F32) + second_in[g, at, :].astype(F32)
            half_out[g, at, :] = value.astype(BF16)
            return carry

        lax.fori_loop(0, half // 64, add, 0)
        for c in final_copies(p):
            c.start()

    count = len(order)
    for p in range(count + 3):
        if p < count:
            if p == 2:
                relay(1, 2)
            if p == 3:
                relay(1, 3)
            down(p)
        if 1 <= p <= count:
            combine(p - 1)
        if 3 <= p:
            merge(p - 3)
    for p in range(count):
        last(p)
    with jax.named_scope("final_wait"):
        for p in range(count):
            here, there = final_copies(p)
            here.wait()
            there.wait()

    for swap in swaps:
        swap.wait_send()

    @pl.when(sp < n_sp - 1)
    def _():
        for c in halo(0, (up_to, t)):
            c.wait_send()

    @pl.when(sp > 0)
    def _():
        for c in halo(1, (down_to, t)):
            c.wait_send()

    for w in range(2):
        for k in range(3):
            first_copy(w, k).wait_send()
        for c in sent[w]:
            c.wait_send()
    for r in range(rounds):
        for k in range(2):
            token_copy(k, r).wait_send()
        token_relay(r).wait_send()
        for k in range(4):
            pair_copy(k, t, r).wait_send()
    for p in range(count):
        twin_copy(block_of(p)).wait_send()
        first_sum(p).wait_send()
        second_sum(p).wait_send()


def extended(x, sides, width):
    for axis, dim in sides:
        count, length = (lax.axis_size(axis), x.shape[dim])
        up = [(i, (i + 1) % count) for i in range(count - 1)]
        down = [(j, i) for i, j in up]
        last = lax.slice_in_dim(x, length - width, length, axis=dim)
        initial = lax.slice_in_dim(x, 0, width, axis=dim)
        before = lax.ppermute(last, axis, up)
        after = lax.ppermute(initial, axis, down)
        x = jnp.concatenate([before, x, after], axis=dim)
    return x


def rms_scale(field, gain):
    wide = field.astype(jnp.float32)
    return wide * lax.rsqrt(jnp.mean(wide * wide, axis=-1, keepdims=True) + EPS) * gain


def mixer_partial(normed, w_up, w_down):
    upward = jnp.dot(
        normed, lax.all_gather(w_up, "sp", axis=0, tiled=True), preferred_element_type=jnp.float32
    )
    active = jnp.square(jax.nn.relu(upward)).astype(jnp.bfloat16)
    return jnp.dot(
        active, lax.all_gather(w_down, "sp", axis=1, tiled=True), preferred_element_type=jnp.float32
    )


def plain_shards(
    resid, queries, keys, values, documents, q_gain, k_gain, sink, w_out, n_gain, w_up, w_down
):
    rows = resid.shape[0]
    head_size = q_gain.shape[0]
    heads_here = sink.shape[0]
    kv_here = keys.shape[1] // head_size
    group = heads_here // kv_here
    qnorm = rms_scale(queries.reshape(rows, kv_here, group, head_size), q_gain).astype(jnp.bfloat16)
    knorm = rms_scale(keys.reshape(rows, kv_here, head_size), k_gain).astype(jnp.bfloat16)
    vheads = values.reshape(rows, kv_here, head_size)
    doc_here = documents.astype(jnp.bfloat16)
    near_keys, near_values, near_docs = (
        extended(knorm, (("sp", 0),), WINDOW),
        extended(vheads, (("sp", 0),), WINDOW),
        extended(doc_here, (("sp", 0),), WINDOW),
    )
    offset = lax.axis_index("sp") * rows
    total = rows * lax.axis_size("sp")
    query_pos = offset + jnp.arange(rows, dtype=jnp.int32)
    key_pos = offset - WINDOW + jnp.arange(rows + 2 * WINDOW, dtype=jnp.int32)
    distance = key_pos[None, :] - query_pos[:, None]
    allowed = (jnp.abs(distance) <= WINDOW) & (key_pos[None, :] >= 0) & (key_pos[None, :] < total)
    allowed = allowed & (near_docs[None, :] == doc_here[:, None])
    heads_all = heads_here * lax.axis_size("tp")
    first_head = (lax.axis_index("tp") * heads_here).astype(jnp.float32)
    slopes = jnp.exp2(
        -8.0 * (first_head + jnp.arange(heads_here, dtype=jnp.float32) + 1.0) / heads_all
    )
    slopes = slopes.reshape(kv_here, group)
    sink_f = sink.reshape(kv_here, group)
    scores = jnp.einsum(
        "rkgd,skd->kgrs", qnorm, near_keys, preferred_element_type=jnp.float32
    ) * head_size ** (-0.5)
    scores = scores - slopes[:, :, None, None] * jnp.abs(distance).astype(jnp.float32)[None, None]
    scores = jnp.where(allowed[None, None], scores, jnp.float32(-1e30))
    highest = jnp.maximum(jnp.max(scores, axis=-1), sink_f[:, :, None])
    weights = jnp.exp(scores - highest[..., None])
    denom = jnp.sum(weights, axis=-1) + jnp.exp(sink_f[:, :, None] - highest)
    summed = jnp.einsum(
        "kgrs,skd->rkgd",
        weights.astype(jnp.bfloat16),
        near_values,
        preferred_element_type=jnp.float32,
    )
    attended = (
        (summed / denom.transpose(2, 0, 1)[..., None])
        .astype(jnp.bfloat16)
        .reshape(rows, heads_here * head_size)
    )
    head_mix = lax.psum(
        jnp.dot(attended, w_out, preferred_element_type=jnp.float32).astype(jnp.bfloat16), "tp"
    ).astype(jnp.float32)
    middle = (resid.astype(jnp.float32) + head_mix).astype(jnp.bfloat16)
    normed = rms_scale(middle, n_gain).astype(jnp.bfloat16)
    partial_sum = mixer_partial(normed, w_up, w_down)
    unit_mix = lax.psum(partial_sum.astype(jnp.bfloat16), "tp").astype(jnp.float32)
    return (middle.astype(jnp.float32) + unit_mix).astype(jnp.bfloat16)


def fused_shards(
    resid, queries, keys, values, documents, q_gain, k_gain, sink, w_out, n_gain, w_up, w_down
):
    rows, width = resid.shape
    half = rows // 2
    n_sp = lax.axis_size("sp")
    head = q_gain.shape[0]
    heads = sink.shape[0]
    kv_heads = keys.shape[1] // head
    units = w_up.shape[1] // MEMBERS
    n_za = n_sp // 8
    rounds = half // WINDOW
    heads_all = heads * lax.axis_size("tp")
    slopes = tuple(2.0 ** (-8.0 * (h + 1.0) / heads_all) for h in range(heads_all))
    vmem = pl.BlockSpec(memory_space=pltpu.VMEM)
    smem = pl.BlockSpec(memory_space=pltpu.SMEM)
    hbm = pl.BlockSpec(memory_space=pl.ANY)
    sends = 3 + 4 * n_za + 4 * (n_za - 1)
    block = 2 * w_down.shape[1]
    blocks = width // block
    dma = pltpu.SemaphoreType.DMA
    return pl.pallas_call(
        functools.partial(kernel, n_sp, head, heads, kv_heads, slopes),
        out_shape=jax.ShapeDtypeStruct((rows, width), BF16),
        in_specs=[hbm, hbm, hbm, hbm, hbm, vmem, vmem, smem, hbm, vmem, hbm, hbm],
        out_specs=hbm,
        scratch_shapes=[
            pltpu.VMEM((rows, heads * head), BF16),
            pltpu.VMEM((rows + 2 * WINDOW, keys.shape[1]), BF16),
            pltpu.VMEM((rows + 2 * WINDOW, keys.shape[1]), BF16),
            pltpu.VMEM((1, rows + 2 * WINDOW), jnp.int32),
            pltpu.VMEM((rows + 2 * WINDOW, keys.shape[1]), BF16),
            pltpu.VMEM((rows, heads * head), BF16),
            pltpu.VMEM(w_out.shape, BF16),
            pltpu.VMEM((half, width), BF16),
            pltpu.VMEM((rounds, 2 * WINDOW, width), BF16),
            pltpu.VMEM((rounds, WINDOW, width), BF16),
            pltpu.VMEM((half, width), BF16),
            pltpu.VMEM((MEMBERS * rows, width), BF16),
            pltpu.VMEM((width, units), BF16),
            pltpu.VMEM((units, width), BF16),
            pltpu.VMEM((MEMBERS * rows, units), BF16),
            pltpu.VMEM((2, MEMBERS, half, block), F32),
            pltpu.VMEM((blocks, MEMBERS, half, block), BF16),
            pltpu.VMEM((blocks, MEMBERS, half, block), BF16),
            pltpu.VMEM((blocks, 2, half, block), BF16),
            pltpu.VMEM((blocks, 2, half, block), BF16),
            pltpu.VMEM((blocks, half, block), BF16),
            pltpu.VMEM((blocks, half, block), BF16),
            pltpu.VMEM((blocks, half, block), F32),
            pltpu.VMEM((blocks, half, block), F32),
            pltpu.VMEM((blocks, half, block), BF16),
            dma((2, 3)),
            dma((2, 3)),
            dma((2, sends)),
            dma((2, n_sp)),
            dma((2,)),
            dma((6,)),
            dma((3, rounds)),
            dma((3, rounds)),
            dma((4, rounds)),
            dma((4, rounds)),
            dma((rounds,)),
            dma((rounds,)),
            dma((blocks,)),
            dma((blocks,)),
            dma((2, blocks)),
            dma((2, blocks)),
            dma((blocks,)),
            dma((blocks,)),
            dma((blocks,)),
        ],
        compiler_params=pltpu.CompilerParams(
            collective_id=0, has_side_effects=True, vmem_limit_bytes=63 * 1024 * 1024
        ),
        name="layer",
    )(
        resid,
        queries,
        keys,
        values,
        documents[None, :],
        q_gain[None, :],
        k_gain[None, :],
        sink,
        w_out,
        n_gain[None, :],
        w_up,
        w_down,
    )


def solution(mesh):
    placed = (
        P("sp", None),
        P("sp", "tp"),
        P("sp", "tp"),
        P("sp", "tp"),
        P("sp"),
        P(),
        P(),
        P("tp"),
        P("tp", None),
        P(),
        P("sp", "tp"),
        P("tp", "sp"),
    )
    sizes = dict(mesh.shape)

    def shards(*args):
        columns = args[11].shape[1]
        fits = sizes["tp"] == 2 and sizes["sp"] % 8 == 0 and columns % 128 == 0
        return (fused_shards if fits else plain_shards)(*args)

    return jax.shard_map(
        shards, mesh=mesh, in_specs=placed, out_specs=P("sp", None), check_vma=False
    )
```

```python
import functools

import jax
import jax.numpy as jnp
from jax import lax
from jax.experimental import pallas as pl
from jax.experimental.pallas import tpu as pltpu
from jax.sharding import PartitionSpec as P

WINDOW = 128
EPS = 1e-06
MEMBERS = 4
F32 = jnp.float32
BF16 = jnp.bfloat16
MESH = pl.DeviceIdType.MESH


def rms(wide, gain):
    return wide * lax.rsqrt(jnp.mean(wide * wide, axis=-1, keepdims=True) + EPS) * gain


def kernel(
    n_sp,
    head,
    heads,
    kv_heads,
    slopes,
    resid,
    queries,
    keys,
    values,
    docs,
    q_gain,
    k_gain,
    sink,
    w_out,
    n_gain,
    w_up,
    w_down,
    out,
    q,
    kx,
    vx,
    dx,
    kn,
    att,
    wo,
    res,
    mixed,
    other_in,
    mid,
    normed,
    wu,
    wd,
    act,
    part,
    twin_out,
    twin_in,
    first_out,
    first_in,
    second_out,
    second_in,
    waiting,
    total,
    half_out,
    halo_send,
    halo_recv,
    w_send,
    w_recv,
    w_local,
    loc_sem,
    tok_send,
    tok_recv,
    pair_send,
    pair_recv,
    swap_send,
    swap_recv,
    twin_send,
    twin_recv,
    sum_send,
    sum_recv,
    fin_send,
    fin_recv,
    fin_local,
    credit,
):
    rows = queries.shape[0]
    half = rows // 2
    depth = w_up.shape[0]
    units = wu.shape[1]
    width = wd.shape[1]
    group = heads // kv_heads
    n_za = n_sp // 8
    block = 2 * w_down.shape[1]

    sp = lax.axis_index("sp")
    t = lax.axis_index("tp")
    u = 1 - t
    x = sp % 2
    y = (sp // 2) % 2
    zb = (sp // 4) % 2
    za = sp // 8
    me = zb * 2 + x

    def index(za_, zb_, y_, x_):
        return za_ * 8 + zb_ * 4 + y_ * 2 + x_

    def flip(v, by):
        return 1 - v if by else v

    def remote(src, dst, send, recv, where):
        return pltpu.make_async_remote_copy(
            src_ref=src, dst_ref=dst, send_sem=send, recv_sem=recv,
            device_id=where, device_id_type=MESH,
        )

    own_q = pltpu.make_async_copy(queries, q, loc_sem.at[5])
    own_k = pltpu.make_async_copy(keys, kx.at[pl.ds(WINDOW, rows), :], loc_sem.at[2])
    own_v = pltpu.make_async_copy(values, vx.at[pl.ds(WINDOW, rows), :], loc_sem.at[3])
    own_d = pltpu.make_async_copy(docs, dx.at[:, pl.ds(WINDOW, rows)], loc_sem.at[4])
    own_k.start()
    own_d.start()
    own_q.start()
    own_v.start()

    up_to = lax.rem(sp + 1, n_sp)
    down_to = lax.rem(sp + n_sp - 1, n_sp)
    flips = ((0, 1), (1, 0), (1, 1))
    near = [(index(za, flip(zb, fz), y, flip(x, fx)), t) for fz, fx in flips]
    across = (index(za, zb, 1 - y, x), t)
    partners = [(sp, u), (up_to, t), (down_to, t), across] + near
    partners += [(index(1 - za, zb_, y, x_), t) for zb_, x_ in ((zb, x), (1 - zb, x), (1 - zb, 1 - x))]
    opposite = partners[-3:]
    inner = za + zb == 1
    with jax.named_scope("barrier"):
        greeting = pltpu.get_barrier_semaphore()
        for where in partners:
            pl.semaphore_signal(greeting, inc=1, device_id=where, device_id_type=MESH)
        pl.semaphore_wait(greeting, len(partners))

    def halo(side, where):
        src = rows - WINDOW if side == 0 else 0
        dst = 0 if side == 0 else WINDOW + rows
        return [
            remote(keys.at[pl.ds(src, WINDOW), :], kx.at[pl.ds(dst, WINDOW), :],
                   halo_send.at[side, 0], halo_recv.at[side, 0], where),
            remote(docs.at[:, pl.ds(src, WINDOW)], dx.at[:, pl.ds(dst, WINDOW)],
                   halo_send.at[side, 2], halo_recv.at[side, 2], where),
            remote(values.at[pl.ds(src, WINDOW), :], vx.at[pl.ds(dst, WINDOW), :],
                   halo_send.at[side, 1], halo_recv.at[side, 1], where),
        ]

    @pl.when(sp < n_sp - 1)
    def _():
        for c in halo(0, (up_to, t)):
            c.start()

    @pl.when(sp > 0)
    def _():
        for c in halo(1, (down_to, t)):
            c.start()

    def place(w, s):
        if w == 0:
            return wu.at[pl.ds(pl.multiple_of(s * depth, depth), depth), :]
        return wd.at[:, pl.ds(pl.multiple_of(s * (block // 2), block // 2), block // 2)]

    def source(w, m):
        at = pl.ds(pl.multiple_of(m * units, units), units)
        return w_up.at[:, at] if w == 0 else w_down.at[at, :]

    def first_copy(w, k):
        fz, fx = flips[k]
        return remote(source(w, flip(zb, fz) * 2 + flip(x, fx)), place(w, sp), w_send.at[w, k],
                      w_recv.at[w, sp], near[k])

    locals_ = [pltpu.make_async_copy(source(w, me), place(w, sp), w_local.at[w]) for w in range(2)]

    def arrived(w, s):
        remote(place(w, s), place(w, s), w_send.at[w, 0], w_recv.at[w, s], (sp, u)).wait_recv()

    sent = [[], []]

    def start(w, s, where, src=None, only=None):
        c = remote(place(w, s) if src is None else src, place(w, s), w_send.at[w, 3 + len(sent[w])],
                   w_recv.at[w, s], where)
        if only is None:
            c.start()
        else:
            pl.when(only)(c.start)
        sent[w].append((c, only))

    def direct(w, i):
        start(w, sp, opposite[1 + i], source(w, (1 - zb) * 2 + (1 - x if i else x)), inner)

    def along(w, k, only=None):
        zb_, x_ = member_at(k)
        start(w, index(za, zb_, y, x_), opposite[0], source(w, me) if k == 0 else None, only)

    def gather(w, k):
        with jax.named_scope(f"gather#w={w}#k={k}"):
            zb_, x_ = member_at(k)
            arrived(w, index(za, zb_, y, x_))

    def member_at(k):
        fz, fx = (0, 0) if k == 0 else flips[k - 1]
        return flip(zb, fz), flip(x, fx)

    def cross(w, k):
        zb_, x_ = member_at(k)
        start(w, index(za, zb_, y, x_), across, source(w, me) if k == 0 else None)

    def relay(w, k):
        with jax.named_scope(f"relay#w={w}#k={k}"):
            zb_, x_ = member_at(k)
            s = index(1 - za, zb_, y, x_)
            arrived(w, s)
            start(w, s, across)

    for k in range(3):
        first_copy(0, k).start()
    locals_[0].start()
    along(0, 0)
    cross(0, 0)
    direct(0, 0)
    direct(0, 1)
    locals_[1].start()
    load_wo = pltpu.make_async_copy(w_out, wo, loc_sem.at[0])
    load_wo.start()
    load_res = pltpu.make_async_copy(resid.at[pl.ds(t * half, half), :], res, loc_sem.at[1])
    load_res.start()

    with jax.named_scope("own_wait"):
        own_k.wait()
        own_v.wait()
        own_d.wait()
        own_q.wait()

    @pl.when(sp > 0)
    def _():
        for c in halo(0, (down_to, t)):
            c.wait_recv()

    @pl.when(sp == 0)
    def _():
        kx[pl.ds(0, WINDOW), :] = jnp.zeros((WINDOW, kx.shape[1]), BF16)
        vx[pl.ds(0, WINDOW), :] = jnp.zeros((WINDOW, vx.shape[1]), BF16)
        dx[:, pl.ds(0, WINDOW)] = jnp.full((1, WINDOW), -1, jnp.int32)

    @pl.when(sp < n_sp - 1)
    def _():
        for c in halo(1, (up_to, t)):
            c.wait_recv()

    @pl.when(sp == n_sp - 1)
    def _():
        end = WINDOW + rows
        kx[pl.ds(end, WINDOW), :] = jnp.zeros((WINDOW, kx.shape[1]), BF16)
        vx[pl.ds(end, WINDOW), :] = jnp.zeros((WINDOW, vx.shape[1]), BF16)
        dx[:, pl.ds(end, WINDOW)] = jnp.full((1, WINDOW), -1, jnp.int32)

    def norm_keys(b, carry):
        at = pl.ds(pl.multiple_of(b * WINDOW, WINDOW), WINDOW)
        wide = kx[at, :].astype(F32)
        kn[at, :] = jnp.concatenate(
            [rms(wide[:, k * head:(k + 1) * head], k_gain[...]) for k in range(kv_heads)], axis=1
        ).astype(BF16)
        return carry

    with jax.named_scope("norm_keys"):
        lax.fori_loop(0, kx.shape[0] // WINDOW, norm_keys, 0)

    span = 3 * WINDOW
    rounds = half // WINDOW

    def attend(b, carry, to):
        at = pl.ds(pl.multiple_of(b * WINDOW, WINDOW), WINDOW)
        put = pl.ds(pl.multiple_of(to * WINDOW, WINDOW), WINDOW)
        window = pl.ds(pl.multiple_of(b * WINDOW, WINDOW), span)
        far = jnp.abs(
            lax.broadcasted_iota(jnp.int32, (WINDOW, span), 1)
            - lax.broadcasted_iota(jnp.int32, (WINDOW, span), 0) - WINDOW
        )
        own = dx[0:1, pl.ds(pl.multiple_of((b + 1) * WINDOW, WINDOW), WINDOW)].astype(F32)
        own = jnp.transpose(jnp.broadcast_to(own, (WINDOW, WINDOW)))[:, 0:1]
        allowed = (far <= WINDOW) & (dx[0:1, window].astype(F32) == own)
        mask = jnp.where(allowed, F32(0.0), F32(-1e30))
        far = far.astype(F32)
        for k in range(kv_heads):
            lanes = slice(k * head, (k + 1) * head)
            kb = kn[window, lanes]
            vb = vx[window, lanes]
            done = []
            for g in range(group):
                h = k * group + g
                slope = jnp.where(t == 0, F32(slopes[h]), F32(slopes[heads + h]))
                qb = rms(q[at, h * head:(h + 1) * head].astype(F32), q_gain[...]).astype(BF16)
                score = lax.dot_general(
                    qb, kb, (((1,), (1,)), ((), ())), preferred_element_type=F32
                ) * (head ** -0.5)
                score = (score - slope * far) + mask
                top = jnp.maximum(jnp.max(score, axis=-1, keepdims=True), sink[h])
                p = jnp.exp(score - top)
                denom = jnp.sum(p, axis=-1, keepdims=True) + jnp.exp(sink[h] - top)
                summed = jnp.dot(p.astype(BF16), vb, preferred_element_type=F32)
                done.append((summed / denom).astype(BF16))
                if len(done) == 2:
                    att[put, (h - 1) * head:(h + 1) * head] = jnp.concatenate(done, axis=1)
                    done = []
        return carry

    tile = 256
    swaps = []

    def project(r):
        lhs = att[pl.ds(r * 2 * WINDOW, 2 * WINDOW), :]

        def step(j, carry):
            cols = pl.ds(pl.multiple_of(j * tile, tile), tile)
            mixed[r, :, cols] = jnp.dot(lhs, wo[:, cols], preferred_element_type=F32).astype(BF16)
            return carry

        lax.fori_loop(0, width // tile, step, 0)

    def token_rows(slot, r):
        return normed.at[pl.ds(pl.multiple_of(slot * half + r * WINDOW, WINDOW), WINDOW), :]

    def token_copy(k, r):
        rows_ = token_rows(me * 2 + t, r)
        return remote(rows_, rows_, tok_send.at[k, r], tok_recv.at[k, r], near[k])

    def member(k):
        if k == 3:
            return me
        fz, fx = flips[k]
        return flip(zb, fz) * 2 + flip(x, fx)

    def pair_copy(k, core, r):
        rows_ = token_rows(member(k) * 2 + core, r)
        return remote(rows_, rows_, pair_send.at[k, r], pair_recv.at[k, r], (sp, u))

    def token_pass(k, r):
        with jax.named_scope(f"token#k={k}#r={r}"):
            rows_ = token_rows(member(k) * 2 + t, r)
            remote(rows_, rows_, tok_send.at[k, r], tok_recv.at[k, r], (sp, u)).wait_recv()
            if k == 1:
                token_relay(r).start()
            pair_copy(k, t, r).start()

    def token_relay(r):
        rows_ = token_rows(member(1) * 2 + t, r)
        return remote(rows_, rows_, tok_send.at[2, r], tok_recv.at[2, r], near[0])

    def one_round(r):
        with jax.named_scope("project"):
            project(r)
            swap = remote(mixed.at[r, pl.ds(pl.multiple_of(u * WINDOW, WINDOW), WINDOW), :], other_in.at[r],
                          swap_send.at[r], swap_recv.at[r], (sp, u))
            swap.start()
            swaps.append(swap)
        with jax.named_scope("swap_wait"):
            swap.wait_recv()

        def middle(i, carry):
            at = pl.ds(pl.multiple_of(i * 64, 64), 64)
            mine = pl.ds(pl.multiple_of(t * WINDOW + i * 64, 64), 64)
            here = pl.ds(pl.multiple_of(r * WINDOW + i * 64, 64), 64)
            both = mixed[r, mine, :].astype(F32) + other_in[r, at, :].astype(F32)
            value = (res[here, :].astype(F32) + both).astype(BF16)
            mid[here, :] = value
            row = pl.multiple_of((me * 2 + t) * half + r * WINDOW + i * 64, 64)
            normed[pl.ds(row, 64), :] = rms(value.astype(F32), n_gain[...]).astype(BF16)
            return carry

        with jax.named_scope("middle"):
            lax.fori_loop(0, WINDOW // 64, middle, 0)
        for k in (1, 0):
            token_copy(k, r).start()
        pair_copy(3, t, r).start()

    def attend_block(r, i):
        with jax.named_scope("attend"):
            lax.fori_loop(0, 1, lambda _, c: attend(r + i * rounds, c, 2 * r + i), 0)

    for r in range(rounds):
        attend_block(r, 0)
        if r == 0:
            gather(0, 1)
            along(0, 1)
            cross(0, 1)
            for k in range(3):
                first_copy(1, k).start()
        if r == 1:
            relay(0, 0)
            relay(0, 1)
        attend_block(r, 1)
        if r == 0:
            for k in (2, 3):
                gather(0, k)
                along(0, k, inner)
                cross(0, k)
            load_wo.wait()
            load_res.wait()
        one_round(r)
        if r == 0:
            direct(1, 0)

    def up(m):
        row = pl.multiple_of(m * rows, rows)

        def step(j, carry):
            cols = pl.ds(pl.multiple_of(j * tile, tile), tile)
            v = jnp.dot(normed[pl.ds(row, rows), :], wu[:, cols], preferred_element_type=F32)
            v = jnp.maximum(v, 0.0)
            act[pl.ds(row, rows), cols] = (v * v).astype(BF16)
            return carry

        with jax.named_scope("up"):
            lax.fori_loop(0, units // tile, step, 0)

    def pair_wait(k):
        with jax.named_scope("pair_wait"):
            for r in range(rounds):
                pair_copy(k, u, r).wait_recv()

    def finish_up():
        with jax.named_scope("finish_up"):
            locals_[0].wait()
            for a in range(n_za):
                for k in range(4):
                    arrived(0, index(a, k // 2, 1 - y, k % 2))

    outer = jnp.logical_not(inner)
    gather(1, 1)
    for k in (0, 1):
        along(1, k, outer)
    if rounds < 2:
        relay(0, 0)
        relay(0, 1)
    relay(0, 2)
    relay(0, 3)
    for k in (0, 1):
        cross(1, k)
    token_pass(1, 0)
    for k in (2, 3):
        gather(1, k)
        cross(1, k)
    for r in range(1, rounds):
        token_pass(1, r)
    direct(1, 1)

    @pl.when(outer)
    def _():
        pl.semaphore_signal(credit, inc=1, device_id=opposite[0], device_id_type=MESH)

    finish_up()
    pair_wait(3)
    up(me)
    for r in range(rounds):
        token_pass(0, r)
    pair_wait(0)
    up(member(0))
    with jax.named_scope("credit_wait"):
        @pl.when(inner)
        def _():
            pl.semaphore_wait(credit, 1)

    for k in range(4):
        along(1, k, inner)
    for r in range(rounds):
        token_pass(2, r)
        if r == 0:
            relay(1, 0)
    for k in (1, 2):
        pair_wait(k)
        up(member(k))
        if k == 1:
            relay(1, 1)
    locals_[1].wait()

    order = [(d, fz, fy) for d in range(n_za) for fy in range(2) for fz in range(2)]
    chunks = 4
    ways = ((0, 1), (1, 0))

    def block_of(p):
        d, fz, fy = order[p]
        return lax.rem(za + n_za - d, n_za) * 4 + flip(zb, fz) * 2 + flip(y, fy)

    def axes(p):
        return ways[0] if order[p][0] % 2 == 0 else ways[1]

    def cols_of(g):
        return pl.ds(pl.multiple_of(g * block, block), block)

    def twin_copy(g):
        return remote(twin_out.at[g], twin_in.at[g], twin_send.at[g], twin_recv.at[g], (sp, u))

    def first_sum(p):
        g = block_of(p)
        return remote(first_out.at[g], first_in.at[g], sum_send.at[0, g], sum_recv.at[0, g], near[axes(p)[0]])

    def second_sum(p):
        g = block_of(p)
        return remote(second_out.at[g], second_in.at[g], sum_send.at[1, g], sum_recv.at[1, g], near[axes(p)[1]])

    def down(p):
        d, fz, fy = order[p]
        g = block_of(p)
        with jax.named_scope(f"down_wait#p={p}"):
            if fy == 1:
                for i in range(2):
                    arrived(1, g * 2 + i)
        cols = cols_of(g)

        def step(c, carry):
            cz, cx = c // 2, c % 2
            row = (zb + cz - 2 * zb * cz) * 2 + (x + cx - 2 * x * cx)
            theirs = pl.ds(pl.multiple_of(row * rows + u * half, half), half)
            ours = pl.ds(pl.multiple_of(row * rows + t * half, half), half)
            twin_out[g, c, :, :] = jnp.dot(act[theirs, :], wd[:, cols], preferred_element_type=F32).astype(BF16)
            part[p % 2, c, :, :] = jnp.dot(act[ours, :], wd[:, cols], preferred_element_type=F32)
            return carry

        with jax.named_scope("down"):
            lax.fori_loop(0, chunks, step, 0)
        twin_copy(g).start()

    def combine(p):
        g = block_of(p)
        cols = cols_of(g)
        one, two = axes(p)
        with jax.named_scope("twin_wait"):
            twin_copy(g).wait_recv()

        def add(i, carry):
            at = pl.ds(pl.multiple_of(i * 64, 64), 64)

            def whole(c):
                return part[p % 2, c, at, :] + twin_in[g, c, at, :].astype(F32)

            first_out[g, 0, at, :] = whole(3).astype(BF16)
            first_out[g, 1, at, :] = whole(one + 1).astype(BF16)
            waiting[g, at, :] = whole(two + 1)
            total[g, at, :] = whole(0) + mid[at, cols].astype(F32)
            return carry

        with jax.named_scope("combine"):
            lax.fori_loop(0, half // 64, add, 0)
        first_sum(p).start()

    def merge(p):
        g = block_of(p)
        with jax.named_scope(f"merge_wait#p={p}"):
            first_sum(p).wait_recv()

        def add(i, carry):
            at = pl.ds(pl.multiple_of(i * 64, 64), 64)
            second_out[g, at, :] = (waiting[g, at, :] + first_in[g, 0, at, :].astype(F32)).astype(BF16)
            return carry

        lax.fori_loop(0, half // 64, add, 0)
        second_sum(p).start()

    def final_copies(p):
        g = block_of(p)
        cols = cols_of(g)
        mine = pl.ds(pl.multiple_of(t * half, half), half)
        return (
            pltpu.make_async_copy(half_out.at[g], out.at[mine, cols], fin_local.at[g]),
            remote(half_out.at[g], out.at[mine, cols], fin_send.at[g], fin_recv.at[g], (sp, u)),
        )

    def last(p):
        g = block_of(p)
        with jax.named_scope(f"sum_wait#p={p}"):
            second_sum(p).wait_recv()

        def add(i, carry):
            at = pl.ds(pl.multiple_of(i * 64, 64), 64)
            value = total[g, at, :] + first_in[g, 1, at, :].astype(F32) + second_in[g, at, :].astype(F32)
            half_out[g, at, :] = value.astype(BF16)
            return carry

        lax.fori_loop(0, half // 64, add, 0)
        for c in final_copies(p):
            c.start()

    count = len(order)
    early = count // 2
    for p in range(early):
        down(p)
        if p:
            combine(p - 1)
        if p == 0:
            relay(1, 2)
        if p == 2:
            relay(1, 3)
    for p in range(early, count):
        down(p)
        combine(p - 1)
        merge(p - early)
    combine(count - 1)
    for p in range(early, count):
        merge(p)
    for p in range(count):
        last(p)
    with jax.named_scope("final_wait"):
        for p in range(count):
            here, there = final_copies(p)
            here.wait()
            there.wait()

    for swap in swaps:
        swap.wait_send()

    @pl.when(sp < n_sp - 1)
    def _():
        for c in halo(0, (up_to, t)):
            c.wait_send()

    @pl.when(sp > 0)
    def _():
        for c in halo(1, (down_to, t)):
            c.wait_send()

    for w in range(2):
        for k in range(3):
            first_copy(w, k).wait_send()
        for c, only in sent[w]:
            if only is None:
                c.wait_send()
            else:
                pl.when(only)(c.wait_send)
    for r in range(rounds):
        for k in range(2):
            token_copy(k, r).wait_send()
        token_relay(r).wait_send()
        for k in range(4):
            pair_copy(k, t, r).wait_send()
    for p in range(count):
        twin_copy(block_of(p)).wait_send()
        first_sum(p).wait_send()
        second_sum(p).wait_send()


def extended(x, sides, width):
    for axis, dim in sides:
        count, length = (lax.axis_size(axis), x.shape[dim])
        up = [(i, (i + 1) % count) for i in range(count - 1)]
        down = [(j, i) for i, j in up]
        last = lax.slice_in_dim(x, length - width, length, axis=dim)
        initial = lax.slice_in_dim(x, 0, width, axis=dim)
        before = lax.ppermute(last, axis, up)
        after = lax.ppermute(initial, axis, down)
        x = jnp.concatenate([before, x, after], axis=dim)
    return x


def rms_scale(field, gain):
    wide = field.astype(jnp.float32)
    return wide * lax.rsqrt(jnp.mean(wide * wide, axis=-1, keepdims=True) + EPS) * gain


def mixer_partial(normed, w_up, w_down):
    upward = jnp.dot(
        normed, lax.all_gather(w_up, "sp", axis=0, tiled=True), preferred_element_type=jnp.float32
    )
    active = jnp.square(jax.nn.relu(upward)).astype(jnp.bfloat16)
    return jnp.dot(
        active, lax.all_gather(w_down, "sp", axis=1, tiled=True), preferred_element_type=jnp.float32
    )


def plain_shards(
    resid, queries, keys, values, documents, q_gain, k_gain, sink, w_out, n_gain, w_up, w_down
):
    rows = resid.shape[0]
    head_size = q_gain.shape[0]
    heads_here = sink.shape[0]
    kv_here = keys.shape[1] // head_size
    group = heads_here // kv_here
    qnorm = rms_scale(queries.reshape(rows, kv_here, group, head_size), q_gain).astype(jnp.bfloat16)
    knorm = rms_scale(keys.reshape(rows, kv_here, head_size), k_gain).astype(jnp.bfloat16)
    vheads = values.reshape(rows, kv_here, head_size)
    doc_here = documents.astype(jnp.bfloat16)
    near_keys, near_values, near_docs = (
        extended(knorm, (("sp", 0),), WINDOW),
        extended(vheads, (("sp", 0),), WINDOW),
        extended(doc_here, (("sp", 0),), WINDOW),
    )
    offset = lax.axis_index("sp") * rows
    total = rows * lax.axis_size("sp")
    query_pos = offset + jnp.arange(rows, dtype=jnp.int32)
    key_pos = offset - WINDOW + jnp.arange(rows + 2 * WINDOW, dtype=jnp.int32)
    distance = key_pos[None, :] - query_pos[:, None]
    allowed = (jnp.abs(distance) <= WINDOW) & (key_pos[None, :] >= 0) & (key_pos[None, :] < total)
    allowed = allowed & (near_docs[None, :] == doc_here[:, None])
    heads_all = heads_here * lax.axis_size("tp")
    first_head = (lax.axis_index("tp") * heads_here).astype(jnp.float32)
    slopes = jnp.exp2(
        -8.0 * (first_head + jnp.arange(heads_here, dtype=jnp.float32) + 1.0) / heads_all
    )
    slopes = slopes.reshape(kv_here, group)
    sink_f = sink.reshape(kv_here, group)
    scores = jnp.einsum(
        "rkgd,skd->kgrs", qnorm, near_keys, preferred_element_type=jnp.float32
    ) * head_size ** (-0.5)
    scores = scores - slopes[:, :, None, None] * jnp.abs(distance).astype(jnp.float32)[None, None]
    scores = jnp.where(allowed[None, None], scores, jnp.float32(-1e30))
    highest = jnp.maximum(jnp.max(scores, axis=-1), sink_f[:, :, None])
    weights = jnp.exp(scores - highest[..., None])
    denom = jnp.sum(weights, axis=-1) + jnp.exp(sink_f[:, :, None] - highest)
    summed = jnp.einsum(
        "kgrs,skd->rkgd",
        weights.astype(jnp.bfloat16),
        near_values,
        preferred_element_type=jnp.float32,
    )
    attended = (
        (summed / denom.transpose(2, 0, 1)[..., None])
        .astype(jnp.bfloat16)
        .reshape(rows, heads_here * head_size)
    )
    head_mix = lax.psum(
        jnp.dot(attended, w_out, preferred_element_type=jnp.float32).astype(jnp.bfloat16), "tp"
    ).astype(jnp.float32)
    middle = (resid.astype(jnp.float32) + head_mix).astype(jnp.bfloat16)
    normed = rms_scale(middle, n_gain).astype(jnp.bfloat16)
    partial_sum = mixer_partial(normed, w_up, w_down)
    unit_mix = lax.psum(partial_sum.astype(jnp.bfloat16), "tp").astype(jnp.float32)
    return (middle.astype(jnp.float32) + unit_mix).astype(jnp.bfloat16)


def fused_shards(
    resid, queries, keys, values, documents, q_gain, k_gain, sink, w_out, n_gain, w_up, w_down
):
    rows, width = resid.shape
    half = rows // 2
    n_sp = lax.axis_size("sp")
    head = q_gain.shape[0]
    heads = sink.shape[0]
    kv_heads = keys.shape[1] // head
    units = w_up.shape[1] // MEMBERS
    n_za = n_sp // 8
    rounds = half // WINDOW
    heads_all = heads * lax.axis_size("tp")
    slopes = tuple(2.0 ** (-8.0 * (h + 1.0) / heads_all) for h in range(heads_all))
    vmem = pl.BlockSpec(memory_space=pltpu.VMEM)
    smem = pl.BlockSpec(memory_space=pltpu.SMEM)
    hbm = pl.BlockSpec(memory_space=pl.ANY)
    sends = 20
    block = 2 * w_down.shape[1]
    blocks = width // block
    dma = pltpu.SemaphoreType.DMA
    return pl.pallas_call(
        functools.partial(kernel, n_sp, head, heads, kv_heads, slopes),
        out_shape=jax.ShapeDtypeStruct((rows, width), BF16),
        in_specs=[hbm, hbm, hbm, hbm, hbm, vmem, vmem, smem, hbm, vmem, hbm, hbm],
        out_specs=hbm,
        scratch_shapes=[
            pltpu.VMEM((rows, heads * head), BF16),
            pltpu.VMEM((rows + 2 * WINDOW, keys.shape[1]), BF16),
            pltpu.VMEM((rows + 2 * WINDOW, keys.shape[1]), BF16),
            pltpu.VMEM((1, rows + 2 * WINDOW), jnp.int32),
            pltpu.VMEM((rows + 2 * WINDOW, keys.shape[1]), BF16),
            pltpu.VMEM((rows, heads * head), BF16),
            pltpu.VMEM(w_out.shape, BF16),
            pltpu.VMEM((half, width), BF16),
            pltpu.VMEM((rounds, 2 * WINDOW, width), BF16),
            pltpu.VMEM((rounds, WINDOW, width), BF16),
            pltpu.VMEM((half, width), BF16),
            pltpu.VMEM((MEMBERS * rows, width), BF16),
            pltpu.VMEM((width, units), BF16),
            pltpu.VMEM((units, width), BF16),
            pltpu.VMEM((MEMBERS * rows, units), BF16),
            pltpu.VMEM((2, MEMBERS, half, block), F32),
            pltpu.VMEM((blocks, MEMBERS, half, block), BF16),
            pltpu.VMEM((blocks, MEMBERS, half, block), BF16),
            pltpu.VMEM((blocks, 2, half, block), BF16),
            pltpu.VMEM((blocks, 2, half, block), BF16),
            pltpu.VMEM((blocks, half, block), BF16),
            pltpu.VMEM((blocks, half, block), BF16),
            pltpu.VMEM((blocks, half, block), F32),
            pltpu.VMEM((blocks, half, block), F32),
            pltpu.VMEM((blocks, half, block), BF16),
            dma((2, 3)),
            dma((2, 3)),
            dma((2, sends)),
            dma((2, n_sp)),
            dma((2,)),
            dma((6,)),
            dma((3, rounds)),
            dma((3, rounds)),
            dma((4, rounds)),
            dma((4, rounds)),
            dma((rounds,)),
            dma((rounds,)),
            dma((blocks,)),
            dma((blocks,)),
            dma((2, blocks)),
            dma((2, blocks)),
            dma((blocks,)),
            dma((blocks,)),
            dma((blocks,)),
            pltpu.SemaphoreType.REGULAR,
        ],
        compiler_params=pltpu.CompilerParams(
            collective_id=0, has_side_effects=True, vmem_limit_bytes=63 * 1024 * 1024
        ),
        name="layer",
    )(
        resid,
        queries,
        keys,
        values,
        documents[None, :],
        q_gain[None, :],
        k_gain[None, :],
        sink,
        w_out,
        n_gain[None, :],
        w_up,
        w_down,
    )


def solution(mesh):
    placed = (
        P("sp", None),
        P("sp", "tp"),
        P("sp", "tp"),
        P("sp", "tp"),
        P("sp"),
        P(),
        P(),
        P("tp"),
        P("tp", None),
        P(),
        P("sp", "tp"),
        P("tp", "sp"),
    )
    sizes = dict(mesh.shape)

    def shards(*args):
        columns = args[11].shape[1]
        fits = sizes["tp"] == 2 and sizes["sp"] // 8 == 2 and sizes["sp"] % 8 == 0 and columns % 128 == 0
        return (fused_shards if fits else plain_shards)(*args)

    return jax.shard_map(
        shards, mesh=mesh, in_specs=placed, out_specs=P("sp", None), check_vma=False
    )
```

```python
import functools

import jax
import jax.numpy as jnp
from jax import lax
from jax.experimental import pallas as pl
from jax.experimental.pallas import tpu as pltpu
from jax.sharding import PartitionSpec as P

WINDOW = 128
EPS = 1e-06
MEMBERS = 4
F32 = jnp.float32
BF16 = jnp.bfloat16
MESH = pl.DeviceIdType.MESH


def rms(wide, gain):
    return wide * lax.rsqrt(jnp.mean(wide * wide, axis=-1, keepdims=True) + EPS) * gain


def kernel(
    n_sp,
    head,
    heads,
    kv_heads,
    slopes,
    resid,
    queries,
    keys,
    values,
    docs,
    q_gain,
    k_gain,
    sink,
    w_out,
    n_gain,
    w_up,
    w_down,
    out,
    q,
    kx,
    vx,
    dx,
    kn,
    att,
    wo,
    res,
    mixed,
    other_in,
    mid,
    normed,
    wu,
    wd,
    act,
    part,
    twin_out,
    twin_in,
    first_out,
    first_in,
    second_out,
    second_in,
    waiting,
    total,
    half_out,
    halo_send,
    halo_recv,
    w_send,
    w_recv,
    w_local,
    loc_sem,
    tok_send,
    tok_recv,
    pair_send,
    pair_recv,
    swap_send,
    swap_recv,
    twin_send,
    twin_recv,
    sum_send,
    sum_recv,
    fin_send,
    fin_recv,
    fin_local,
    credit,
):
    rows = queries.shape[0]
    half = rows // 2
    depth = w_up.shape[0]
    units = wu.shape[1]
    width = resid.shape[1]
    group = heads // kv_heads
    n_za = n_sp // 8
    block = 2 * w_down.shape[1]

    sp = lax.axis_index("sp")
    t = lax.axis_index("tp")
    u = 1 - t
    x = sp % 2
    y = (sp // 2) % 2
    zb = (sp // 4) % 2
    za = sp // 8
    me = zb * 2 + x

    def index(za_, zb_, y_, x_):
        return za_ * 8 + zb_ * 4 + y_ * 2 + x_

    def flip(v, by):
        return 1 - v if by else v

    def remote(src, dst, send, recv, where):
        return pltpu.make_async_remote_copy(
            src_ref=src, dst_ref=dst, send_sem=send, recv_sem=recv,
            device_id=where, device_id_type=MESH,
        )

    own_q = pltpu.make_async_copy(queries, q, loc_sem.at[5])
    own_k = pltpu.make_async_copy(keys, kx.at[pl.ds(WINDOW, rows), :], loc_sem.at[2])
    own_v = pltpu.make_async_copy(values, vx.at[pl.ds(WINDOW, rows), :], loc_sem.at[3])
    own_d = pltpu.make_async_copy(docs, dx.at[:, pl.ds(WINDOW, rows)], loc_sem.at[4])
    own_k.start()
    own_d.start()
    own_q.start()
    own_v.start()

    up_to = lax.rem(sp + 1, n_sp)
    down_to = lax.rem(sp + n_sp - 1, n_sp)
    flips = ((0, 1), (1, 0), (1, 1))
    near = [(index(za, flip(zb, fz), y, flip(x, fx)), t) for fz, fx in flips]
    across = (index(za, zb, 1 - y, x), t)
    partners = [(sp, u), (up_to, t), (down_to, t), across] + near
    partners += [(index(1 - za, zb_, y, x_), t) for zb_, x_ in ((zb, x), (1 - zb, x), (1 - zb, 1 - x))]
    opposite = partners[-3:]
    inner = za + zb == 1
    with jax.named_scope("barrier"):
        greeting = pltpu.get_barrier_semaphore()
        for where in partners:
            pl.semaphore_signal(greeting, inc=1, device_id=where, device_id_type=MESH)
        pl.semaphore_wait(greeting, len(partners))

    def halo(side, where):
        src = rows - WINDOW if side == 0 else 0
        dst = 0 if side == 0 else WINDOW + rows
        return [
            remote(keys.at[pl.ds(src, WINDOW), :], kx.at[pl.ds(dst, WINDOW), :],
                   halo_send.at[side, 0], halo_recv.at[side, 0], where),
            remote(docs.at[:, pl.ds(src, WINDOW)], dx.at[:, pl.ds(dst, WINDOW)],
                   halo_send.at[side, 2], halo_recv.at[side, 2], where),
            remote(values.at[pl.ds(src, WINDOW), :], vx.at[pl.ds(dst, WINDOW), :],
                   halo_send.at[side, 1], halo_recv.at[side, 1], where),
        ]

    @pl.when(sp < n_sp - 1)
    def _():
        for c in halo(0, (up_to, t)):
            c.start()

    @pl.when(sp > 0)
    def _():
        for c in halo(1, (down_to, t)):
            c.start()

    def place(w, s):
        if w == 0:
            return wu.at[pl.ds(pl.multiple_of(s * depth, depth), depth), :]
        return wd.at[s]

    def source(w, m):
        at = pl.ds(pl.multiple_of(m * units, units), units)
        return w_up.at[:, at] if w == 0 else w_down.at[at, :]

    def first_copy(w, k):
        fz, fx = flips[k]
        return remote(source(w, flip(zb, fz) * 2 + flip(x, fx)), place(w, sp), w_send.at[w, k],
                      w_recv.at[w, sp], near[k])

    locals_ = [pltpu.make_async_copy(source(w, me), place(w, sp), w_local.at[w]) for w in range(2)]

    def arrived(w, s):
        remote(place(w, s), place(w, s), w_send.at[w, 0], w_recv.at[w, s], (sp, u)).wait_recv()

    sent = [[], []]

    def start(w, s, where, src=None, only=None):
        c = remote(place(w, s) if src is None else src, place(w, s), w_send.at[w, 3 + len(sent[w])],
                   w_recv.at[w, s], where)
        if only is None:
            c.start()
        else:
            pl.when(only)(c.start)
        sent[w].append((c, only))

    def direct(w, i):
        start(w, sp, opposite[1 + i], source(w, (1 - zb) * 2 + (1 - x if i else x)), inner)

    def along(w, k, only=None):
        zb_, x_ = member_at(k)
        start(w, index(za, zb_, y, x_), opposite[0], source(w, me) if k == 0 else None, only)

    def gather(w, k):
        with jax.named_scope(f"gather#w={w}#k={k}"):
            zb_, x_ = member_at(k)
            arrived(w, index(za, zb_, y, x_))

    def member_at(k):
        fz, fx = (0, 0) if k == 0 else flips[k - 1]
        return flip(zb, fz), flip(x, fx)

    def cross(w, k):
        zb_, x_ = member_at(k)
        start(w, index(za, zb_, y, x_), across, source(w, me) if k == 0 else None)

    def relay(w, k):
        with jax.named_scope(f"relay#w={w}#k={k}"):
            zb_, x_ = member_at(k)
            s = index(1 - za, zb_, y, x_)
            arrived(w, s)
            start(w, s, across)

    for k in range(3):
        first_copy(0, k).start()
    locals_[0].start()
    along(0, 0)
    cross(0, 0)
    direct(0, 0)
    direct(0, 1)
    locals_[1].start()
    load_wo = pltpu.make_async_copy(w_out, wo, loc_sem.at[0])
    load_wo.start()
    load_res = pltpu.make_async_copy(resid.at[pl.ds(t * half, half), :], res, loc_sem.at[1])
    load_res.start()

    with jax.named_scope("own_wait"):
        own_k.wait()
        own_v.wait()
        own_d.wait()
        own_q.wait()

    @pl.when(sp > 0)
    def _():
        for c in halo(0, (down_to, t)):
            c.wait_recv()

    @pl.when(sp == 0)
    def _():
        kx[pl.ds(0, WINDOW), :] = jnp.zeros((WINDOW, kx.shape[1]), BF16)
        vx[pl.ds(0, WINDOW), :] = jnp.zeros((WINDOW, vx.shape[1]), BF16)
        dx[:, pl.ds(0, WINDOW)] = jnp.full((1, WINDOW), -1, jnp.int32)

    @pl.when(sp < n_sp - 1)
    def _():
        for c in halo(1, (up_to, t)):
            c.wait_recv()

    @pl.when(sp == n_sp - 1)
    def _():
        end = WINDOW + rows
        kx[pl.ds(end, WINDOW), :] = jnp.zeros((WINDOW, kx.shape[1]), BF16)
        vx[pl.ds(end, WINDOW), :] = jnp.zeros((WINDOW, vx.shape[1]), BF16)
        dx[:, pl.ds(end, WINDOW)] = jnp.full((1, WINDOW), -1, jnp.int32)

    def norm_keys(b, carry):
        at = pl.ds(pl.multiple_of(b * WINDOW, WINDOW), WINDOW)
        wide = kx[at, :].astype(F32)
        kn[at, :] = jnp.concatenate(
            [rms(wide[:, k * head:(k + 1) * head], k_gain[...]) for k in range(kv_heads)], axis=1
        ).astype(BF16)
        return carry

    with jax.named_scope("norm_keys"):
        lax.fori_loop(0, kx.shape[0] // WINDOW, norm_keys, 0)

    span = 3 * WINDOW
    rounds = half // WINDOW

    def attend(b, carry, to):
        at = pl.ds(pl.multiple_of(b * WINDOW, WINDOW), WINDOW)
        put = pl.ds(pl.multiple_of(to * WINDOW, WINDOW), WINDOW)
        window = pl.ds(pl.multiple_of(b * WINDOW, WINDOW), span)
        far = jnp.abs(
            lax.broadcasted_iota(jnp.int32, (WINDOW, span), 1)
            - lax.broadcasted_iota(jnp.int32, (WINDOW, span), 0) - WINDOW
        )
        own = dx[0:1, pl.ds(pl.multiple_of((b + 1) * WINDOW, WINDOW), WINDOW)].astype(F32)
        own = jnp.transpose(jnp.broadcast_to(own, (WINDOW, WINDOW)))[:, 0:1]
        allowed = (far <= WINDOW) & (dx[0:1, window].astype(F32) == own)
        mask = jnp.where(allowed, F32(0.0), F32(-1e30))
        far = far.astype(F32)
        for k in range(kv_heads):
            lanes = slice(k * head, (k + 1) * head)
            kb = kn[window, lanes]
            vb = vx[window, lanes]
            done = []
            for g in range(group):
                h = k * group + g
                slope = jnp.where(t == 0, F32(slopes[h]), F32(slopes[heads + h]))
                qb = rms(q[at, h * head:(h + 1) * head].astype(F32), q_gain[...]).astype(BF16)
                score = lax.dot_general(
                    qb, kb, (((1,), (1,)), ((), ())), preferred_element_type=F32
                ) * (head ** -0.5)
                score = (score - slope * far) + mask
                top = jnp.maximum(jnp.max(score, axis=-1, keepdims=True), sink[h])
                p = jnp.exp(score - top)
                denom = jnp.sum(p, axis=-1, keepdims=True) + jnp.exp(sink[h] - top)
                summed = jnp.dot(p.astype(BF16), vb, preferred_element_type=F32)
                done.append((summed / denom).astype(BF16))
                if len(done) == 2:
                    att[put, (h - 1) * head:(h + 1) * head] = jnp.concatenate(done, axis=1)
                    done = []
        return carry

    tile = 256
    swaps = []

    def project(r):
        lhs = att[pl.ds(r * 2 * WINDOW, 2 * WINDOW), :]

        def step(j, carry):
            cols = pl.ds(pl.multiple_of(j * tile, tile), tile)
            mixed[r, :, cols] = jnp.dot(lhs, wo[:, cols], preferred_element_type=F32).astype(BF16)
            return carry

        lax.fori_loop(0, width // tile, step, 0)

    def token_rows(slot, r):
        return normed.at[pl.ds(pl.multiple_of(slot * half + r * WINDOW, WINDOW), WINDOW), :]

    def token_copy(k, r):
        rows_ = token_rows(me * 2 + t, r)
        return remote(rows_, rows_, tok_send.at[k, r], tok_recv.at[k, r], near[k])

    def member(k):
        if k == 3:
            return me
        fz, fx = flips[k]
        return flip(zb, fz) * 2 + flip(x, fx)

    def pair_copy(k, core, r):
        rows_ = token_rows(member(k) * 2 + core, r)
        return remote(rows_, rows_, pair_send.at[k, r], pair_recv.at[k, r], (sp, u))

    def token_pass(k, r):
        with jax.named_scope(f"token#k={k}#r={r}"):
            rows_ = token_rows(member(k) * 2 + t, r)
            remote(rows_, rows_, tok_send.at[k, r], tok_recv.at[k, r], (sp, u)).wait_recv()
            if k == 1:
                token_relay(r).start()
            pair_copy(k, t, r).start()

    def token_relay(r):
        rows_ = token_rows(member(1) * 2 + t, r)
        return remote(rows_, rows_, tok_send.at[2, r], tok_recv.at[2, r], near[0])

    def one_round(r):
        with jax.named_scope("project"):
            project(r)
            swap = remote(mixed.at[r, pl.ds(pl.multiple_of(u * WINDOW, WINDOW), WINDOW), :], other_in.at[r],
                          swap_send.at[r], swap_recv.at[r], (sp, u))
            swap.start()
            swaps.append(swap)
        with jax.named_scope("swap_wait"):
            swap.wait_recv()

        def middle(i, carry):
            at = pl.ds(pl.multiple_of(i * 64, 64), 64)
            mine = pl.ds(pl.multiple_of(t * WINDOW + i * 64, 64), 64)
            here = pl.ds(pl.multiple_of(r * WINDOW + i * 64, 64), 64)
            both = mixed[r, mine, :].astype(F32) + other_in[r, at, :].astype(F32)
            value = (res[here, :].astype(F32) + both).astype(BF16)
            mid[here, :] = value
            row = pl.multiple_of((me * 2 + t) * half + r * WINDOW + i * 64, 64)
            normed[pl.ds(row, 64), :] = rms(value.astype(F32), n_gain[...]).astype(BF16)
            return carry

        with jax.named_scope("middle"):
            lax.fori_loop(0, WINDOW // 64, middle, 0)
        for k in (1, 0):
            token_copy(k, r).start()
        pair_copy(3, t, r).start()

    def attend_block(r, i):
        with jax.named_scope("attend"):
            lax.fori_loop(0, 1, lambda _, c: attend(r + i * rounds, c, 2 * r + i), 0)

    for r in range(rounds):
        attend_block(r, 0)
        if r == 0:
            gather(0, 1)
            along(0, 1)
            cross(0, 1)
            for k in range(3):
                first_copy(1, k).start()
        if r == 1:
            relay(0, 0)
            relay(0, 1)
        attend_block(r, 1)
        if r == 0:
            for k in (2, 3):
                gather(0, k)
                along(0, k, inner)
                cross(0, k)
            load_wo.wait()
            load_res.wait()
        one_round(r)
        if r == 0:
            direct(1, 0)

    def up(m):
        row = pl.multiple_of(m * rows, rows)

        def step(j, carry):
            cols = pl.ds(pl.multiple_of(j * tile, tile), tile)
            v = jnp.dot(normed[pl.ds(row, rows), :], wu[:, cols], preferred_element_type=F32)
            v = jnp.maximum(v, 0.0)
            act[pl.ds(row, rows), cols] = (v * v).astype(BF16)
            return carry

        with jax.named_scope("up"):
            lax.fori_loop(0, units // tile, step, 0)

    def pair_wait(k):
        with jax.named_scope("pair_wait"):
            for r in range(rounds):
                pair_copy(k, u, r).wait_recv()

    def finish_up():
        with jax.named_scope("finish_up"):
            locals_[0].wait()
            for a in range(n_za):
                for k in range(4):
                    arrived(0, index(a, k // 2, 1 - y, k % 2))

    outer = jnp.logical_not(inner)
    gather(1, 1)
    for k in (0, 1):
        along(1, k, outer)
    if rounds < 2:
        relay(0, 0)
        relay(0, 1)
    relay(0, 2)
    relay(0, 3)
    for k in (0, 1):
        cross(1, k)
    token_pass(1, 0)
    for k in (2, 3):
        gather(1, k)
        cross(1, k)
    for r in range(1, rounds):
        token_pass(1, r)
    direct(1, 1)

    @pl.when(outer)
    def _():
        pl.semaphore_signal(credit, inc=1, device_id=opposite[0], device_id_type=MESH)

    finish_up()
    pair_wait(3)
    up(me)
    for r in range(rounds):
        token_pass(0, r)
    pair_wait(0)
    up(member(0))
    with jax.named_scope("credit_wait"):
        @pl.when(inner)
        def _():
            pl.semaphore_wait(credit, 1)

    for k in range(4):
        along(1, k, inner)
    order = [(d, fz, fy) for d in range(n_za) for fy in range(2) for fz in range(2)]
    ways = ((0, 1), (1, 0))

    def block_of(p):
        d, fz, fy = order[p]
        return lax.rem(za + n_za - d, n_za) * 4 + flip(zb, fz) * 2 + flip(y, fy)

    def axes(p):
        return ways[1] if p >= len(order) - 2 else ways[0]

    def cols_of(g):
        return pl.ds(pl.multiple_of(g * block, block), block)

    def twin_copy(p, z):
        at = (block_of(p), pl.ds(2 * z, 2))
        return remote(twin_out.at[at], twin_in.at[at], twin_send.at[z, block_of(p)],
                      twin_recv.at[z, block_of(p)], (sp, u))

    def first_sum(p, i):
        g = block_of(p)
        return remote(first_out.at[g, i], first_in.at[g, i], sum_send.at[i, g], sum_recv.at[i, g],
                      near[axes(p)[0]])

    def second_sum(p):
        g = block_of(p)
        return remote(second_out.at[g], second_in.at[g], sum_send.at[2, g], sum_recv.at[2, g], near[axes(p)[1]])

    pending = []
    passes = [0]

    def down(p, z):
        g = block_of(p)
        slot = passes[0] % 3
        passes[0] += 1
        if z == 0 and order[p][2] == 1:
            with jax.named_scope(f"down_wait#p={p}"):
                for i in range(2):
                    arrived(1, g * 2 + i)
        zb_ = flip(zb, z)

        def step(c, carry):
            row = zb_ * 2 + (x + c - 2 * x * c)
            theirs = pl.ds(pl.multiple_of(row * rows + u * half, half), half)
            ours = pl.ds(pl.multiple_of(row * rows + t * half, half), half)
            cols = jnp.concatenate([wd[g * 2], wd[g * 2 + 1]], axis=1)
            twin_out[g, 2 * z + c, :, :] = jnp.dot(act[theirs, :], cols, preferred_element_type=F32).astype(BF16)
            part[slot, c, :, :] = jnp.dot(act[ours, :], cols, preferred_element_type=F32)
            return carry

        with jax.named_scope("down"):
            lax.fori_loop(0, 2, step, 0)
        twin_copy(p, z).start()
        pending.append((p, z, slot))
        if len(pending) > 2:
            combine(*pending.pop(0))

    def flush():
        while pending:
            combine(*pending.pop(0))

    def combine(p, z, slot):
        g = block_of(p)
        cols = cols_of(g)
        x_first = axes(p)[0] == 0
        with jax.named_scope("twin_wait"):
            twin_copy(p, z).wait_recv()

        def add(i, carry):
            at = pl.ds(pl.multiple_of(i * 64, 64), 64)

            def whole(c):
                return part[slot, c, at, :] + twin_in[g, 2 * z + c, at, :].astype(F32)

            if z == 0:
                total[g, at, :] = whole(0) + mid[at, cols].astype(F32)
            else:
                first_out[g, 0, at, :] = whole(1).astype(BF16)
            if x_first == (z == 0):
                first_out[g, 1, at, :] = whole(1 - z).astype(BF16)
            else:
                waiting[g, at, :] = whole(1 - z)
            return carry

        with jax.named_scope("combine"):
            lax.fori_loop(0, half // 64, add, 0)
        if z == 1:
            first_sum(p, 0).start()
        if x_first == (z == 0):
            first_sum(p, 1).start()

    def merge(p):
        g = block_of(p)
        with jax.named_scope(f"merge_wait#p={p}"):
            first_sum(p, 0).wait_recv()

        def add(i, carry):
            at = pl.ds(pl.multiple_of(i * 64, 64), 64)
            second_out[g, at, :] = (waiting[g, at, :] + first_in[g, 0, at, :].astype(F32)).astype(BF16)
            return carry

        lax.fori_loop(0, half // 64, add, 0)
        second_sum(p).start()

    def final_copies(p):
        g = block_of(p)
        cols = cols_of(g)
        mine = pl.ds(pl.multiple_of(t * half, half), half)
        return (
            pltpu.make_async_copy(half_out.at[g], out.at[mine, cols], fin_local.at[g]),
            remote(half_out.at[g], out.at[mine, cols], fin_send.at[g], fin_recv.at[g], (sp, u)),
        )

    def last(p):
        g = block_of(p)
        with jax.named_scope(f"sum_wait#p={p}"):
            first_sum(p, 1).wait_recv()
            second_sum(p).wait_recv()

        def add(i, carry):
            at = pl.ds(pl.multiple_of(i * 64, 64), 64)
            value = total[g, at, :] + first_in[g, 1, at, :].astype(F32) + second_in[g, at, :].astype(F32)
            half_out[g, at, :] = value.astype(BF16)
            return carry

        lax.fori_loop(0, half // 64, add, 0)
        for c in final_copies(p):
            c.start()

    count = len(order)
    early = count // 2
    locals_[1].wait()
    down(0, 0)
    down(1, 0)
    token_pass(2, 0)
    down(2, 0)
    down(3, 0)
    flush()
    relay(1, 0)
    for r in range(1, rounds):
        token_pass(2, r)
    pair_wait(1)
    up(member(1))
    relay(1, 1)
    pair_wait(2)
    up(member(2))
    relay(1, 2)
    for p in range(early):
        down(p, 1)
        if p == 1:
            relay(1, 3)
    for p in range(early, count):
        down(p, 0)
        down(p, 1)
        merge(p - early)
    flush()
    for p in range(early, count):
        merge(p)
    for p in range(count):
        last(p)
    with jax.named_scope("final_wait"):
        for p in range(count):
            here, there = final_copies(p)
            here.wait()
            there.wait()

    for swap in swaps:
        swap.wait_send()

    @pl.when(sp < n_sp - 1)
    def _():
        for c in halo(0, (up_to, t)):
            c.wait_send()

    @pl.when(sp > 0)
    def _():
        for c in halo(1, (down_to, t)):
            c.wait_send()

    for w in range(2):
        for k in range(3):
            first_copy(w, k).wait_send()
        for c, only in sent[w]:
            if only is None:
                c.wait_send()
            else:
                pl.when(only)(c.wait_send)
    for r in range(rounds):
        for k in range(2):
            token_copy(k, r).wait_send()
        token_relay(r).wait_send()
        for k in range(4):
            pair_copy(k, t, r).wait_send()
    for p in range(count):
        for i in range(2):
            twin_copy(p, i).wait_send()
            first_sum(p, i).wait_send()
        second_sum(p).wait_send()


def extended(x, sides, width):
    for axis, dim in sides:
        count, length = (lax.axis_size(axis), x.shape[dim])
        up = [(i, (i + 1) % count) for i in range(count - 1)]
        down = [(j, i) for i, j in up]
        last = lax.slice_in_dim(x, length - width, length, axis=dim)
        initial = lax.slice_in_dim(x, 0, width, axis=dim)
        before = lax.ppermute(last, axis, up)
        after = lax.ppermute(initial, axis, down)
        x = jnp.concatenate([before, x, after], axis=dim)
    return x


def rms_scale(field, gain):
    wide = field.astype(jnp.float32)
    return wide * lax.rsqrt(jnp.mean(wide * wide, axis=-1, keepdims=True) + EPS) * gain


def mixer_partial(normed, w_up, w_down):
    upward = jnp.dot(
        normed, lax.all_gather(w_up, "sp", axis=0, tiled=True), preferred_element_type=jnp.float32
    )
    active = jnp.square(jax.nn.relu(upward)).astype(jnp.bfloat16)
    return jnp.dot(
        active, lax.all_gather(w_down, "sp", axis=1, tiled=True), preferred_element_type=jnp.float32
    )


def plain_shards(
    resid, queries, keys, values, documents, q_gain, k_gain, sink, w_out, n_gain, w_up, w_down
):
    rows = resid.shape[0]
    head_size = q_gain.shape[0]
    heads_here = sink.shape[0]
    kv_here = keys.shape[1] // head_size
    group = heads_here // kv_here
    qnorm = rms_scale(queries.reshape(rows, kv_here, group, head_size), q_gain).astype(jnp.bfloat16)
    knorm = rms_scale(keys.reshape(rows, kv_here, head_size), k_gain).astype(jnp.bfloat16)
    vheads = values.reshape(rows, kv_here, head_size)
    doc_here = documents.astype(jnp.bfloat16)
    near_keys, near_values, near_docs = (
        extended(knorm, (("sp", 0),), WINDOW),
        extended(vheads, (("sp", 0),), WINDOW),
        extended(doc_here, (("sp", 0),), WINDOW),
    )
    offset = lax.axis_index("sp") * rows
    total = rows * lax.axis_size("sp")
    query_pos = offset + jnp.arange(rows, dtype=jnp.int32)
    key_pos = offset - WINDOW + jnp.arange(rows + 2 * WINDOW, dtype=jnp.int32)
    distance = key_pos[None, :] - query_pos[:, None]
    allowed = (jnp.abs(distance) <= WINDOW) & (key_pos[None, :] >= 0) & (key_pos[None, :] < total)
    allowed = allowed & (near_docs[None, :] == doc_here[:, None])
    heads_all = heads_here * lax.axis_size("tp")
    first_head = (lax.axis_index("tp") * heads_here).astype(jnp.float32)
    slopes = jnp.exp2(
        -8.0 * (first_head + jnp.arange(heads_here, dtype=jnp.float32) + 1.0) / heads_all
    )
    slopes = slopes.reshape(kv_here, group)
    sink_f = sink.reshape(kv_here, group)
    scores = jnp.einsum(
        "rkgd,skd->kgrs", qnorm, near_keys, preferred_element_type=jnp.float32
    ) * head_size ** (-0.5)
    scores = scores - slopes[:, :, None, None] * jnp.abs(distance).astype(jnp.float32)[None, None]
    scores = jnp.where(allowed[None, None], scores, jnp.float32(-1e30))
    highest = jnp.maximum(jnp.max(scores, axis=-1), sink_f[:, :, None])
    weights = jnp.exp(scores - highest[..., None])
    denom = jnp.sum(weights, axis=-1) + jnp.exp(sink_f[:, :, None] - highest)
    summed = jnp.einsum(
        "kgrs,skd->rkgd",
        weights.astype(jnp.bfloat16),
        near_values,
        preferred_element_type=jnp.float32,
    )
    attended = (
        (summed / denom.transpose(2, 0, 1)[..., None])
        .astype(jnp.bfloat16)
        .reshape(rows, heads_here * head_size)
    )
    head_mix = lax.psum(
        jnp.dot(attended, w_out, preferred_element_type=jnp.float32).astype(jnp.bfloat16), "tp"
    ).astype(jnp.float32)
    middle = (resid.astype(jnp.float32) + head_mix).astype(jnp.bfloat16)
    normed = rms_scale(middle, n_gain).astype(jnp.bfloat16)
    partial_sum = mixer_partial(normed, w_up, w_down)
    unit_mix = lax.psum(partial_sum.astype(jnp.bfloat16), "tp").astype(jnp.float32)
    return (middle.astype(jnp.float32) + unit_mix).astype(jnp.bfloat16)


def fused_shards(
    resid, queries, keys, values, documents, q_gain, k_gain, sink, w_out, n_gain, w_up, w_down
):
    rows, width = resid.shape
    half = rows // 2
    n_sp = lax.axis_size("sp")
    head = q_gain.shape[0]
    heads = sink.shape[0]
    kv_heads = keys.shape[1] // head
    units = w_up.shape[1] // MEMBERS
    n_za = n_sp // 8
    rounds = half // WINDOW
    heads_all = heads * lax.axis_size("tp")
    slopes = tuple(2.0 ** (-8.0 * (h + 1.0) / heads_all) for h in range(heads_all))
    vmem = pl.BlockSpec(memory_space=pltpu.VMEM)
    smem = pl.BlockSpec(memory_space=pltpu.SMEM)
    hbm = pl.BlockSpec(memory_space=pl.ANY)
    sends = 20
    block = 2 * w_down.shape[1]
    blocks = width // block
    dma = pltpu.SemaphoreType.DMA
    return pl.pallas_call(
        functools.partial(kernel, n_sp, head, heads, kv_heads, slopes),
        out_shape=jax.ShapeDtypeStruct((rows, width), BF16),
        in_specs=[hbm, hbm, hbm, hbm, hbm, vmem, vmem, smem, hbm, vmem, hbm, hbm],
        out_specs=hbm,
        scratch_shapes=[
            pltpu.VMEM((rows, heads * head), BF16),
            pltpu.VMEM((rows + 2 * WINDOW, keys.shape[1]), BF16),
            pltpu.VMEM((rows + 2 * WINDOW, keys.shape[1]), BF16),
            pltpu.VMEM((1, rows + 2 * WINDOW), jnp.int32),
            pltpu.VMEM((rows + 2 * WINDOW, keys.shape[1]), BF16),
            pltpu.VMEM((rows, heads * head), BF16),
            pltpu.VMEM(w_out.shape, BF16),
            pltpu.VMEM((half, width), BF16),
            pltpu.VMEM((rounds, 2 * WINDOW, width), BF16),
            pltpu.VMEM((rounds, WINDOW, width), BF16),
            pltpu.VMEM((half, width), BF16),
            pltpu.VMEM((MEMBERS * rows, width), BF16),
            pltpu.VMEM((width, units), BF16),
            pltpu.VMEM((n_sp, units, w_down.shape[1]), BF16),
            pltpu.VMEM((MEMBERS * rows, units), BF16),
            pltpu.VMEM((3, 2, half, block), F32),
            pltpu.VMEM((blocks, MEMBERS, half, block), BF16),
            pltpu.VMEM((blocks, MEMBERS, half, block), BF16),
            pltpu.VMEM((blocks, 2, half, block), BF16),
            pltpu.VMEM((blocks, 2, half, block), BF16),
            pltpu.VMEM((blocks, half, block), BF16),
            pltpu.VMEM((blocks, half, block), BF16),
            pltpu.VMEM((blocks, half, block), F32),
            pltpu.VMEM((blocks, half, block), F32),
            pltpu.VMEM((blocks, half, block), BF16),
            dma((2, 3)),
            dma((2, 3)),
            dma((2, sends)),
            dma((2, n_sp)),
            dma((2,)),
            dma((6,)),
            dma((3, rounds)),
            dma((3, rounds)),
            dma((4, rounds)),
            dma((4, rounds)),
            dma((rounds,)),
            dma((rounds,)),
            dma((2, blocks)),
            dma((2, blocks)),
            dma((3, blocks)),
            dma((3, blocks)),
            dma((blocks,)),
            dma((blocks,)),
            dma((blocks,)),
            pltpu.SemaphoreType.REGULAR,
        ],
        compiler_params=pltpu.CompilerParams(
            collective_id=0, has_side_effects=True, vmem_limit_bytes=63 * 1024 * 1024
        ),
        name="layer",
    )(
        resid,
        queries,
        keys,
        values,
        documents[None, :],
        q_gain[None, :],
        k_gain[None, :],
        sink,
        w_out,
        n_gain[None, :],
        w_up,
        w_down,
    )


def solution(mesh):
    placed = (
        P("sp", None),
        P("sp", "tp"),
        P("sp", "tp"),
        P("sp", "tp"),
        P("sp"),
        P(),
        P(),
        P("tp"),
        P("tp", None),
        P(),
        P("sp", "tp"),
        P("tp", "sp"),
    )
    sizes = dict(mesh.shape)

    def shards(*args):
        columns = args[11].shape[1]
        fits = sizes["tp"] == 2 and sizes["sp"] // 8 == 2 and sizes["sp"] % 8 == 0 and columns % 128 == 0
        return (fused_shards if fits else plain_shards)(*args)

    return jax.shard_map(
        shards, mesh=mesh, in_specs=placed, out_specs=P("sp", None), check_vma=False
    )
```

```python
import functools

import jax
import jax.numpy as jnp
from jax import lax
from jax.experimental import pallas as pl
from jax.experimental.pallas import tpu as pltpu
from jax.sharding import PartitionSpec as P

WINDOW = 128
EPS = 1e-06
MEMBERS = 4
F32 = jnp.float32
BF16 = jnp.bfloat16
MESH = pl.DeviceIdType.MESH


def rms(wide, gain):
    return wide * lax.rsqrt(jnp.mean(wide * wide, axis=-1, keepdims=True) + EPS) * gain


def kernel(
    n_sp,
    head,
    heads,
    kv_heads,
    slopes,
    resid,
    queries,
    keys,
    values,
    docs,
    q_gain,
    k_gain,
    sink,
    w_out,
    n_gain,
    w_up,
    w_down,
    out,
    q,
    kx,
    vx,
    dx,
    kn,
    att,
    wo,
    res,
    mixed,
    other_in,
    mid,
    normed,
    wu,
    wd,
    act,
    part,
    twin_out,
    twin_in,
    first_out,
    first_in,
    second_out,
    second_in,
    waiting,
    total,
    half_out,
    halo_send,
    halo_recv,
    w_send,
    w_recv,
    w_local,
    loc_sem,
    tok_send,
    tok_recv,
    pair_send,
    pair_recv,
    swap_send,
    swap_recv,
    twin_send,
    twin_recv,
    sum_send,
    sum_recv,
    fin_send,
    fin_recv,
    fin_local,
    credit,
):
    rows = queries.shape[0]
    half = rows // 2
    depth = w_up.shape[0]
    units = wu.shape[1]
    width = resid.shape[1]
    group = heads // kv_heads
    n_za = n_sp // 8
    block = 2 * w_down.shape[1]

    sp = lax.axis_index("sp")
    t = lax.axis_index("tp")
    u = 1 - t
    x = sp % 2
    y = (sp // 2) % 2
    zb = (sp // 4) % 2
    za = sp // 8
    me = zb * 2 + x

    def index(za_, zb_, y_, x_):
        return za_ * 8 + zb_ * 4 + y_ * 2 + x_

    def flip(v, by):
        return 1 - v if by else v

    def remote(src, dst, send, recv, where):
        return pltpu.make_async_remote_copy(
            src_ref=src, dst_ref=dst, send_sem=send, recv_sem=recv,
            device_id=where, device_id_type=MESH,
        )

    own_q = pltpu.make_async_copy(queries, q, loc_sem.at[5])
    own_k = pltpu.make_async_copy(keys, kx.at[pl.ds(WINDOW, rows), :], loc_sem.at[2])
    own_v = pltpu.make_async_copy(values, vx.at[pl.ds(WINDOW, rows), :], loc_sem.at[3])
    own_d = pltpu.make_async_copy(docs, dx.at[:, pl.ds(WINDOW, rows)], loc_sem.at[4])
    own_k.start()
    own_d.start()
    own_q.start()
    own_v.start()

    up_to = lax.rem(sp + 1, n_sp)
    down_to = lax.rem(sp + n_sp - 1, n_sp)
    flips = ((0, 1), (1, 0), (1, 1))
    near = [(index(za, flip(zb, fz), y, flip(x, fx)), t) for fz, fx in flips]
    across = (index(za, zb, 1 - y, x), t)
    partners = [(sp, u), (up_to, t), (down_to, t), across] + near
    partners += [(index(1 - za, zb_, y, x_), t) for zb_, x_ in ((zb, x), (1 - zb, x), (1 - zb, 1 - x))]
    opposite = partners[-3:]
    inner = za + zb == 1
    with jax.named_scope("barrier"):
        greeting = pltpu.get_barrier_semaphore()
        for where in partners:
            pl.semaphore_signal(greeting, inc=1, device_id=where, device_id_type=MESH)
        pl.semaphore_wait(greeting, len(partners))

    def halo(side, where):
        src = rows - WINDOW if side == 0 else 0
        dst = 0 if side == 0 else WINDOW + rows
        return [
            remote(keys.at[pl.ds(src, WINDOW), :], kx.at[pl.ds(dst, WINDOW), :],
                   halo_send.at[side, 0], halo_recv.at[side, 0], where),
            remote(docs.at[:, pl.ds(src, WINDOW)], dx.at[:, pl.ds(dst, WINDOW)],
                   halo_send.at[side, 2], halo_recv.at[side, 2], where),
            remote(values.at[pl.ds(src, WINDOW), :], vx.at[pl.ds(dst, WINDOW), :],
                   halo_send.at[side, 1], halo_recv.at[side, 1], where),
        ]

    @pl.when(sp < n_sp - 1)
    def _():
        for c in halo(0, (up_to, t)):
            c.start()

    @pl.when(sp > 0)
    def _():
        for c in halo(1, (down_to, t)):
            c.start()

    def place(w, s):
        if w == 0:
            return wu.at[pl.ds(pl.multiple_of(s * depth, depth), depth), :]
        return wd.at[s]

    def source(w, m):
        at = pl.ds(pl.multiple_of(m * units, units), units)
        return w_up.at[:, at] if w == 0 else w_down.at[at, :]

    def first_copy(w, k):
        fz, fx = flips[k]
        return remote(source(w, flip(zb, fz) * 2 + flip(x, fx)), place(w, sp), w_send.at[w, k],
                      w_recv.at[w, sp], near[k])

    locals_ = [pltpu.make_async_copy(source(w, me), place(w, sp), w_local.at[w]) for w in range(2)]

    def arrived(w, s):
        remote(place(w, s), place(w, s), w_send.at[w, 0], w_recv.at[w, s], (sp, u)).wait_recv()

    sent = [[], []]

    def start(w, s, where, src=None, only=None):
        c = remote(place(w, s) if src is None else src, place(w, s), w_send.at[w, 3 + len(sent[w])],
                   w_recv.at[w, s], where)
        if only is None:
            c.start()
        else:
            pl.when(only)(c.start)
        sent[w].append((c, only))

    def direct(w, i):
        start(w, sp, opposite[1 + i], source(w, (1 - zb) * 2 + (1 - x if i else x)), inner)

    def along(w, k, only=None):
        zb_, x_ = member_at(k)
        start(w, index(za, zb_, y, x_), opposite[0], source(w, me) if k == 0 else None, only)

    def gather(w, k):
        with jax.named_scope(f"gather#w={w}#k={k}"):
            zb_, x_ = member_at(k)
            arrived(w, index(za, zb_, y, x_))

    def member_at(k):
        fz, fx = (0, 0) if k == 0 else flips[k - 1]
        return flip(zb, fz), flip(x, fx)

    def cross(w, k):
        zb_, x_ = member_at(k)
        start(w, index(za, zb_, y, x_), across, source(w, me) if k == 0 else None)

    def relay(w, k):
        with jax.named_scope(f"relay#w={w}#k={k}"):
            zb_, x_ = member_at(k)
            s = index(1 - za, zb_, y, x_)
            arrived(w, s)
            start(w, s, across)

    for k in range(3):
        first_copy(0, k).start()
    locals_[0].start()
    along(0, 0)
    cross(0, 0)
    direct(0, 0)
    direct(0, 1)
    locals_[1].start()
    load_wo = pltpu.make_async_copy(w_out, wo, loc_sem.at[0])
    load_wo.start()
    load_res = pltpu.make_async_copy(resid.at[pl.ds(t * half, half), :], res, loc_sem.at[1])
    load_res.start()

    with jax.named_scope("own_wait"):
        own_k.wait()
        own_v.wait()
        own_d.wait()
        own_q.wait()

    @pl.when(sp > 0)
    def _():
        for c in halo(0, (down_to, t)):
            c.wait_recv()

    @pl.when(sp == 0)
    def _():
        kx[pl.ds(0, WINDOW), :] = jnp.zeros((WINDOW, kx.shape[1]), BF16)
        vx[pl.ds(0, WINDOW), :] = jnp.zeros((WINDOW, vx.shape[1]), BF16)
        dx[:, pl.ds(0, WINDOW)] = jnp.full((1, WINDOW), -1, jnp.int32)

    @pl.when(sp < n_sp - 1)
    def _():
        for c in halo(1, (up_to, t)):
            c.wait_recv()

    @pl.when(sp == n_sp - 1)
    def _():
        end = WINDOW + rows
        kx[pl.ds(end, WINDOW), :] = jnp.zeros((WINDOW, kx.shape[1]), BF16)
        vx[pl.ds(end, WINDOW), :] = jnp.zeros((WINDOW, vx.shape[1]), BF16)
        dx[:, pl.ds(end, WINDOW)] = jnp.full((1, WINDOW), -1, jnp.int32)

    def norm_keys(b, carry):
        at = pl.ds(pl.multiple_of(b * WINDOW, WINDOW), WINDOW)
        wide = kx[at, :].astype(F32)
        kn[at, :] = jnp.concatenate(
            [rms(wide[:, k * head:(k + 1) * head], k_gain[...]) for k in range(kv_heads)], axis=1
        ).astype(BF16)
        return carry

    with jax.named_scope("norm_keys"):
        lax.fori_loop(0, kx.shape[0] // WINDOW, norm_keys, 0)

    span = 3 * WINDOW
    rounds = half // WINDOW

    def attend(b, carry, to):
        at = pl.ds(pl.multiple_of(b * WINDOW, WINDOW), WINDOW)
        put = pl.ds(pl.multiple_of(to * WINDOW, WINDOW), WINDOW)
        window = pl.ds(pl.multiple_of(b * WINDOW, WINDOW), span)
        far = jnp.abs(
            lax.broadcasted_iota(jnp.int32, (WINDOW, span), 1)
            - lax.broadcasted_iota(jnp.int32, (WINDOW, span), 0) - WINDOW
        )
        own = dx[0:1, pl.ds(pl.multiple_of((b + 1) * WINDOW, WINDOW), WINDOW)].astype(F32)
        own = jnp.transpose(jnp.broadcast_to(own, (WINDOW, WINDOW)))[:, 0:1]
        allowed = (far <= WINDOW) & (dx[0:1, window].astype(F32) == own)
        mask = jnp.where(allowed, F32(0.0), F32(-1e30))
        far = far.astype(F32)
        for k in range(kv_heads):
            lanes = slice(k * head, (k + 1) * head)
            kb = kn[window, lanes]
            vb = vx[window, lanes]
            done = []
            for g in range(group):
                h = k * group + g
                slope = jnp.where(t == 0, F32(slopes[h]), F32(slopes[heads + h]))
                qb = rms(q[at, h * head:(h + 1) * head].astype(F32), q_gain[...]).astype(BF16)
                score = lax.dot_general(
                    qb, kb, (((1,), (1,)), ((), ())), preferred_element_type=F32
                ) * (head ** -0.5)
                score = (score - slope * far) + mask
                top = jnp.maximum(jnp.max(score, axis=-1, keepdims=True), sink[h])
                p = jnp.exp(score - top)
                denom = jnp.sum(p, axis=-1, keepdims=True) + jnp.exp(sink[h] - top)
                summed = jnp.dot(p.astype(BF16), vb, preferred_element_type=F32)
                done.append((summed / denom).astype(BF16))
                if len(done) == 2:
                    att[put, (h - 1) * head:(h + 1) * head] = jnp.concatenate(done, axis=1)
                    done = []
        return carry

    tile = 256
    swaps = []

    def project(r):
        lhs = att[pl.ds(r * 2 * WINDOW, 2 * WINDOW), :]

        def step(j, carry):
            cols = pl.ds(pl.multiple_of(j * tile, tile), tile)
            mixed[r, :, cols] = jnp.dot(lhs, wo[:, cols], preferred_element_type=F32).astype(BF16)
            return carry

        lax.fori_loop(0, width // tile, step, 0)

    def token_rows(slot, r):
        return normed.at[pl.ds(pl.multiple_of(slot * half + r * WINDOW, WINDOW), WINDOW), :]

    def token_copy(k, r):
        rows_ = token_rows(me * 2 + t, r)
        return remote(rows_, rows_, tok_send.at[k, r], tok_recv.at[k, r], near[k])

    def member(k):
        if k == 3:
            return me
        fz, fx = flips[k]
        return flip(zb, fz) * 2 + flip(x, fx)

    def pair_copy(k, core, r):
        rows_ = token_rows(member(k) * 2 + core, r)
        return remote(rows_, rows_, pair_send.at[k, r], pair_recv.at[k, r], (sp, u))

    def token_pass(k, r):
        with jax.named_scope(f"token#k={k}#r={r}"):
            rows_ = token_rows(member(k) * 2 + t, r)
            remote(rows_, rows_, tok_send.at[k, r], tok_recv.at[k, r], (sp, u)).wait_recv()
            if k == 1:
                token_relay(r).start()
            pair_copy(k, t, r).start()

    def token_relay(r):
        rows_ = token_rows(member(1) * 2 + t, r)
        return remote(rows_, rows_, tok_send.at[2, r], tok_recv.at[2, r], near[0])

    def one_round(r):
        with jax.named_scope("project"):
            project(r)
            swap = remote(mixed.at[r, pl.ds(pl.multiple_of(u * WINDOW, WINDOW), WINDOW), :], other_in.at[r],
                          swap_send.at[r], swap_recv.at[r], (sp, u))
            swap.start()
            swaps.append(swap)
        with jax.named_scope("swap_wait"):
            swap.wait_recv()

        def middle(i, carry):
            at = pl.ds(pl.multiple_of(i * 64, 64), 64)
            mine = pl.ds(pl.multiple_of(t * WINDOW + i * 64, 64), 64)
            here = pl.ds(pl.multiple_of(r * WINDOW + i * 64, 64), 64)
            both = mixed[r, mine, :].astype(F32) + other_in[r, at, :].astype(F32)
            value = (res[here, :].astype(F32) + both).astype(BF16)
            mid[here, :] = value
            row = pl.multiple_of((me * 2 + t) * half + r * WINDOW + i * 64, 64)
            normed[pl.ds(row, 64), :] = rms(value.astype(F32), n_gain[...]).astype(BF16)
            return carry

        with jax.named_scope("middle"):
            lax.fori_loop(0, WINDOW // 64, middle, 0)
        for k in (1, 0):
            token_copy(k, r).start()
        pair_copy(3, t, r).start()

    def attend_block(r, i):
        with jax.named_scope("attend"):
            lax.fori_loop(0, 1, lambda _, c: attend(r + i * rounds, c, 2 * r + i), 0)

    for r in range(rounds):
        attend_block(r, 0)
        if r == 0:
            gather(0, 1)
            along(0, 1)
            cross(0, 1)
            for k in range(3):
                first_copy(1, k).start()
        if r == 1:
            relay(0, 0)
            relay(0, 1)
        attend_block(r, 1)
        if r == 0:
            for k in (2, 3):
                gather(0, k)
                along(0, k, inner)
                cross(0, k)
            load_wo.wait()
            load_res.wait()
        one_round(r)
        if r == 0:
            direct(1, 0)

    def up(m):
        row = pl.multiple_of(m * rows, rows)

        def step(j, carry):
            cols = pl.ds(pl.multiple_of(j * tile, tile), tile)
            v = jnp.dot(normed[pl.ds(row, rows), :], wu[:, cols], preferred_element_type=F32)
            v = jnp.maximum(v, 0.0)
            act[pl.ds(row, rows), cols] = (v * v).astype(BF16)
            return carry

        with jax.named_scope("up"):
            lax.fori_loop(0, units // tile, step, 0)

    def pair_wait(k):
        with jax.named_scope("pair_wait"):
            for r in range(rounds):
                pair_copy(k, u, r).wait_recv()

    def finish_up():
        with jax.named_scope("finish_up"):
            locals_[0].wait()
            for a in range(n_za):
                for k in range(4):
                    arrived(0, index(a, k // 2, 1 - y, k % 2))

    outer = jnp.logical_not(inner)
    gather(1, 1)
    for k in (0, 1):
        along(1, k, outer)
    if rounds < 2:
        relay(0, 0)
        relay(0, 1)
    relay(0, 2)
    relay(0, 3)
    for k in (0, 1):
        cross(1, k)
    token_pass(1, 0)
    for k in (2, 3):
        gather(1, k)
        cross(1, k)
    for r in range(1, rounds):
        token_pass(1, r)
    direct(1, 1)

    @pl.when(outer)
    def _():
        pl.semaphore_signal(credit, inc=1, device_id=opposite[0], device_id_type=MESH)

    finish_up()
    pair_wait(3)
    up(me)
    for r in range(rounds):
        token_pass(0, r)
    pair_wait(0)
    up(member(0))
    with jax.named_scope("credit_wait"):
        @pl.when(inner)
        def _():
            pl.semaphore_wait(credit, 1)

    for k in range(4):
        along(1, k, inner)
    order = [(d, fz, fy) for d in range(n_za) for fy in range(2) for fz in range(2)]
    ways = ((0, 1), (1, 0))

    def block_of(p):
        d, fz, fy = order[p]
        return lax.rem(za + n_za - d, n_za) * 4 + flip(zb, fz) * 2 + flip(y, fy)

    def axes(p):
        return ways[1] if order[p][0] == 1 and order[p][2] == 0 else ways[0]

    def cols_of(g):
        return pl.ds(pl.multiple_of(g * block, block), block)

    def twin_copy(p, z):
        at = (block_of(p), pl.ds(2 * z, 2))
        return remote(twin_out.at[at], twin_in.at[at], twin_send.at[z, block_of(p)],
                      twin_recv.at[z, block_of(p)], (sp, u))

    def first_sum(p, i):
        g = block_of(p)
        return remote(first_out.at[g, i], first_in.at[g, i], sum_send.at[i, g], sum_recv.at[i, g],
                      near[axes(p)[0]])

    def second_sum(p):
        g = block_of(p)
        return remote(second_out.at[g], second_in.at[g], sum_send.at[2, g], sum_recv.at[2, g], near[axes(p)[1]])

    pending = []
    passes = [0]

    def down(p, z):
        g = block_of(p)
        slot = passes[0] % 3
        passes[0] += 1
        if z == 0 and order[p][2] == 1:
            with jax.named_scope(f"down_wait#p={p}"):
                for i in range(2):
                    arrived(1, g * 2 + i)
        zb_ = flip(zb, z)

        def step(c, carry):
            row = zb_ * 2 + (x + c - 2 * x * c)
            theirs = pl.ds(pl.multiple_of(row * rows + u * half, half), half)
            ours = pl.ds(pl.multiple_of(row * rows + t * half, half), half)
            cols = jnp.concatenate([wd[g * 2], wd[g * 2 + 1]], axis=1)
            twin_out[g, 2 * z + c, :, :] = jnp.dot(act[theirs, :], cols, preferred_element_type=F32).astype(BF16)
            part[slot, c, :, :] = jnp.dot(act[ours, :], cols, preferred_element_type=F32)
            return carry

        with jax.named_scope("down"):
            lax.fori_loop(0, 2, step, 0)
        twin_copy(p, z).start()
        pending.append((p, z, slot))
        if len(pending) > 2:
            combine(*pending.pop(0))

    def flush():
        while pending:
            combine(*pending.pop(0))

    def combine(p, z, slot):
        g = block_of(p)
        cols = cols_of(g)
        x_first = axes(p)[0] == 0
        with jax.named_scope("twin_wait"):
            twin_copy(p, z).wait_recv()

        def add(i, carry):
            at = pl.ds(pl.multiple_of(i * 64, 64), 64)

            def whole(c):
                return part[slot, c, at, :] + twin_in[g, 2 * z + c, at, :].astype(F32)

            if z == 0:
                total[g, at, :] = whole(0) + mid[at, cols].astype(F32)
            else:
                first_out[g, 0, at, :] = whole(1).astype(BF16)
            if x_first == (z == 0):
                first_out[g, 1, at, :] = whole(1 - z).astype(BF16)
            else:
                waiting[g, at, :] = whole(1 - z)
            return carry

        with jax.named_scope("combine"):
            lax.fori_loop(0, half // 64, add, 0)
        if z == 1:
            first_sum(p, 0).start()
        if x_first == (z == 0):
            first_sum(p, 1).start()

    def merge(p):
        g = block_of(p)
        with jax.named_scope(f"merge_wait#p={p}"):
            first_sum(p, 0).wait_recv()

        def add(i, carry):
            at = pl.ds(pl.multiple_of(i * 64, 64), 64)
            second_out[g, at, :] = (waiting[g, at, :] + first_in[g, 0, at, :].astype(F32)).astype(BF16)
            return carry

        lax.fori_loop(0, half // 64, add, 0)
        second_sum(p).start()

    def final_copies(p):
        g = block_of(p)
        cols = cols_of(g)
        mine = pl.ds(pl.multiple_of(t * half, half), half)
        return (
            pltpu.make_async_copy(half_out.at[g], out.at[mine, cols], fin_local.at[g]),
            remote(half_out.at[g], out.at[mine, cols], fin_send.at[g], fin_recv.at[g], (sp, u)),
        )

    def last(p):
        g = block_of(p)
        with jax.named_scope(f"sum_wait#p={p}"):
            first_sum(p, 1).wait_recv()
            second_sum(p).wait_recv()

        def add(i, carry):
            at = pl.ds(pl.multiple_of(i * 64, 64), 64)
            value = total[g, at, :] + first_in[g, 1, at, :].astype(F32) + second_in[g, at, :].astype(F32)
            half_out[g, at, :] = value.astype(BF16)
            return carry

        lax.fori_loop(0, half // 64, add, 0)
        for c in final_copies(p):
            c.start()

    count = len(order)
    early = count // 2
    locals_[1].wait()
    down(0, 0)
    down(1, 0)
    token_pass(2, 0)
    down(2, 0)
    down(3, 0)
    flush()
    relay(1, 0)
    for r in range(1, rounds):
        token_pass(2, r)
    pair_wait(1)
    up(member(1))
    pair_wait(2)
    up(member(2))
    relay(1, 1)
    for p in range(early - 1):
        down(p, 1)
    flush()
    relay(1, 2)
    down(early - 1, 1)
    flush()
    relay(1, 3)
    for p in range(early, count):
        down(p, 0)
        down(p, 1)
        merge(p - early)
    flush()
    late = tuple(range(early + 2, count))
    for p in late[:1] + (early,) + late[1:] + (early + 1,):
        merge(p)
    for p in range(count):
        last(p)
    with jax.named_scope("final_wait"):
        for p in range(count):
            here, there = final_copies(p)
            here.wait()
            there.wait()

    for swap in swaps:
        swap.wait_send()

    @pl.when(sp < n_sp - 1)
    def _():
        for c in halo(0, (up_to, t)):
            c.wait_send()

    @pl.when(sp > 0)
    def _():
        for c in halo(1, (down_to, t)):
            c.wait_send()

    for w in range(2):
        for k in range(3):
            first_copy(w, k).wait_send()
        for c, only in sent[w]:
            if only is None:
                c.wait_send()
            else:
                pl.when(only)(c.wait_send)
    for r in range(rounds):
        for k in range(2):
            token_copy(k, r).wait_send()
        token_relay(r).wait_send()
        for k in range(4):
            pair_copy(k, t, r).wait_send()
    for p in range(count):
        for i in range(2):
            twin_copy(p, i).wait_send()
            first_sum(p, i).wait_send()
        second_sum(p).wait_send()


def extended(x, sides, width):
    for axis, dim in sides:
        count, length = (lax.axis_size(axis), x.shape[dim])
        up = [(i, (i + 1) % count) for i in range(count - 1)]
        down = [(j, i) for i, j in up]
        last = lax.slice_in_dim(x, length - width, length, axis=dim)
        initial = lax.slice_in_dim(x, 0, width, axis=dim)
        before = lax.ppermute(last, axis, up)
        after = lax.ppermute(initial, axis, down)
        x = jnp.concatenate([before, x, after], axis=dim)
    return x


def rms_scale(field, gain):
    wide = field.astype(jnp.float32)
    return wide * lax.rsqrt(jnp.mean(wide * wide, axis=-1, keepdims=True) + EPS) * gain


def mixer_partial(normed, w_up, w_down):
    upward = jnp.dot(
        normed, lax.all_gather(w_up, "sp", axis=0, tiled=True), preferred_element_type=jnp.float32
    )
    active = jnp.square(jax.nn.relu(upward)).astype(jnp.bfloat16)
    return jnp.dot(
        active, lax.all_gather(w_down, "sp", axis=1, tiled=True), preferred_element_type=jnp.float32
    )


def plain_shards(
    resid, queries, keys, values, documents, q_gain, k_gain, sink, w_out, n_gain, w_up, w_down
):
    rows = resid.shape[0]
    head_size = q_gain.shape[0]
    heads_here = sink.shape[0]
    kv_here = keys.shape[1] // head_size
    group = heads_here // kv_here
    qnorm = rms_scale(queries.reshape(rows, kv_here, group, head_size), q_gain).astype(jnp.bfloat16)
    knorm = rms_scale(keys.reshape(rows, kv_here, head_size), k_gain).astype(jnp.bfloat16)
    vheads = values.reshape(rows, kv_here, head_size)
    doc_here = documents.astype(jnp.bfloat16)
    near_keys, near_values, near_docs = (
        extended(knorm, (("sp", 0),), WINDOW),
        extended(vheads, (("sp", 0),), WINDOW),
        extended(doc_here, (("sp", 0),), WINDOW),
    )
    offset = lax.axis_index("sp") * rows
    total = rows * lax.axis_size("sp")
    query_pos = offset + jnp.arange(rows, dtype=jnp.int32)
    key_pos = offset - WINDOW + jnp.arange(rows + 2 * WINDOW, dtype=jnp.int32)
    distance = key_pos[None, :] - query_pos[:, None]
    allowed = (jnp.abs(distance) <= WINDOW) & (key_pos[None, :] >= 0) & (key_pos[None, :] < total)
    allowed = allowed & (near_docs[None, :] == doc_here[:, None])
    heads_all = heads_here * lax.axis_size("tp")
    first_head = (lax.axis_index("tp") * heads_here).astype(jnp.float32)
    slopes = jnp.exp2(
        -8.0 * (first_head + jnp.arange(heads_here, dtype=jnp.float32) + 1.0) / heads_all
    )
    slopes = slopes.reshape(kv_here, group)
    sink_f = sink.reshape(kv_here, group)
    scores = jnp.einsum(
        "rkgd,skd->kgrs", qnorm, near_keys, preferred_element_type=jnp.float32
    ) * head_size ** (-0.5)
    scores = scores - slopes[:, :, None, None] * jnp.abs(distance).astype(jnp.float32)[None, None]
    scores = jnp.where(allowed[None, None], scores, jnp.float32(-1e30))
    highest = jnp.maximum(jnp.max(scores, axis=-1), sink_f[:, :, None])
    weights = jnp.exp(scores - highest[..., None])
    denom = jnp.sum(weights, axis=-1) + jnp.exp(sink_f[:, :, None] - highest)
    summed = jnp.einsum(
        "kgrs,skd->rkgd",
        weights.astype(jnp.bfloat16),
        near_values,
        preferred_element_type=jnp.float32,
    )
    attended = (
        (summed / denom.transpose(2, 0, 1)[..., None])
        .astype(jnp.bfloat16)
        .reshape(rows, heads_here * head_size)
    )
    head_mix = lax.psum(
        jnp.dot(attended, w_out, preferred_element_type=jnp.float32).astype(jnp.bfloat16), "tp"
    ).astype(jnp.float32)
    middle = (resid.astype(jnp.float32) + head_mix).astype(jnp.bfloat16)
    normed = rms_scale(middle, n_gain).astype(jnp.bfloat16)
    partial_sum = mixer_partial(normed, w_up, w_down)
    unit_mix = lax.psum(partial_sum.astype(jnp.bfloat16), "tp").astype(jnp.float32)
    return (middle.astype(jnp.float32) + unit_mix).astype(jnp.bfloat16)


def fused_shards(
    resid, queries, keys, values, documents, q_gain, k_gain, sink, w_out, n_gain, w_up, w_down
):
    rows, width = resid.shape
    half = rows // 2
    n_sp = lax.axis_size("sp")
    head = q_gain.shape[0]
    heads = sink.shape[0]
    kv_heads = keys.shape[1] // head
    units = w_up.shape[1] // MEMBERS
    n_za = n_sp // 8
    rounds = half // WINDOW
    heads_all = heads * lax.axis_size("tp")
    slopes = tuple(2.0 ** (-8.0 * (h + 1.0) / heads_all) for h in range(heads_all))
    vmem = pl.BlockSpec(memory_space=pltpu.VMEM)
    smem = pl.BlockSpec(memory_space=pltpu.SMEM)
    hbm = pl.BlockSpec(memory_space=pl.ANY)
    sends = 20
    block = 2 * w_down.shape[1]
    blocks = width // block
    dma = pltpu.SemaphoreType.DMA
    return pl.pallas_call(
        functools.partial(kernel, n_sp, head, heads, kv_heads, slopes),
        out_shape=jax.ShapeDtypeStruct((rows, width), BF16),
        in_specs=[hbm, hbm, hbm, hbm, hbm, vmem, vmem, smem, hbm, vmem, hbm, hbm],
        out_specs=hbm,
        scratch_shapes=[
            pltpu.VMEM((rows, heads * head), BF16),
            pltpu.VMEM((rows + 2 * WINDOW, keys.shape[1]), BF16),
            pltpu.VMEM((rows + 2 * WINDOW, keys.shape[1]), BF16),
            pltpu.VMEM((1, rows + 2 * WINDOW), jnp.int32),
            pltpu.VMEM((rows + 2 * WINDOW, keys.shape[1]), BF16),
            pltpu.VMEM((rows, heads * head), BF16),
            pltpu.VMEM(w_out.shape, BF16),
            pltpu.VMEM((half, width), BF16),
            pltpu.VMEM((rounds, 2 * WINDOW, width), BF16),
            pltpu.VMEM((rounds, WINDOW, width), BF16),
            pltpu.VMEM((half, width), BF16),
            pltpu.VMEM((MEMBERS * rows, width), BF16),
            pltpu.VMEM((width, units), BF16),
            pltpu.VMEM((n_sp, units, w_down.shape[1]), BF16),
            pltpu.VMEM((MEMBERS * rows, units), BF16),
            pltpu.VMEM((3, 2, half, block), F32),
            pltpu.VMEM((blocks, MEMBERS, half, block), BF16),
            pltpu.VMEM((blocks, MEMBERS, half, block), BF16),
            pltpu.VMEM((blocks, 2, half, block), BF16),
            pltpu.VMEM((blocks, 2, half, block), BF16),
            pltpu.VMEM((blocks, half, block), BF16),
            pltpu.VMEM((blocks, half, block), BF16),
            pltpu.VMEM((blocks, half, block), F32),
            pltpu.VMEM((blocks, half, block), F32),
            pltpu.VMEM((blocks, half, block), BF16),
            dma((2, 3)),
            dma((2, 3)),
            dma((2, sends)),
            dma((2, n_sp)),
            dma((2,)),
            dma((6,)),
            dma((3, rounds)),
            dma((3, rounds)),
            dma((4, rounds)),
            dma((4, rounds)),
            dma((rounds,)),
            dma((rounds,)),
            dma((2, blocks)),
            dma((2, blocks)),
            dma((3, blocks)),
            dma((3, blocks)),
            dma((blocks,)),
            dma((blocks,)),
            dma((blocks,)),
            pltpu.SemaphoreType.REGULAR,
        ],
        compiler_params=pltpu.CompilerParams(
            collective_id=0, has_side_effects=True, vmem_limit_bytes=63 * 1024 * 1024
        ),
        name="layer",
    )(
        resid,
        queries,
        keys,
        values,
        documents[None, :],
        q_gain[None, :],
        k_gain[None, :],
        sink,
        w_out,
        n_gain[None, :],
        w_up,
        w_down,
    )


def solution(mesh):
    placed = (
        P("sp", None),
        P("sp", "tp"),
        P("sp", "tp"),
        P("sp", "tp"),
        P("sp"),
        P(),
        P(),
        P("tp"),
        P("tp", None),
        P(),
        P("sp", "tp"),
        P("tp", "sp"),
    )
    sizes = dict(mesh.shape)

    def shards(*args):
        columns = args[11].shape[1]
        fits = sizes["tp"] == 2 and sizes["sp"] // 8 == 2 and sizes["sp"] % 8 == 0 and columns % 128 == 0
        return (fused_shards if fits else plain_shards)(*args)

    return jax.shard_map(
        shards, mesh=mesh, in_specs=placed, out_specs=P("sp", None), check_vma=False
    )
```
